32 devices in a mesh: sp: 4 (over y, x), dp: 8 (over z, core).
Axes of the slice: x: 2, y: 2, z: 4, core: 2. Of those that a mesh axis runs over, the one named last changes fastest.
Arguments:
- tokens: bfloat16 [8, 1280, 2048], P('dp', 'sp'), may hold values from -6 to 6
- up_weight: bfloat16 [2048, 2048], P('dp'), may hold values from -0.125 to 0.125
- gate_weight: bfloat16 [2048, 2048], P('dp'), may hold values from -0.125 to 0.125
- group_gain: float32 [16, 128], P('sp'), may hold values from 0.1 to 1.9
- mix_weight: bfloat16 [16, 1280, 1280], P('sp', 'dp'), may hold values from -0.15625 to 0.15625
- mix_bias: float32 [16, 1280], P('sp'), may hold values from 0.5 to 1.5
- out_gain: float32 [2048], replicated, may hold values from 0.1 to 1.9
- out_weight: bfloat16 [2048, 2048], P(None, 'dp'), may hold values from -0.125 to 0.125
Outputs:
- mixed_out: bfloat16 [8, 1280, 2048], P('dp', 'sp')
The draws below stay inside these ranges and needn't reach their ends.
All inputs are finite; a program needn't handle non-finite values.
Results may differ from the reference program's by a relative error of at most 0.0072.
Values may be sent and summed in bfloat16 or wider, within the bound.
A program may use at most 128 MiB of HBM per device.

```python
import jax
import jax.numpy as jnp
from jax import lax

D = 2048
GROUPS = 16
GROUP_DIM = 128
SPAN = 1280
WIDTH = 2048
LENGTH = 1280
SEQS = 8


def level_of(key, extent, cuts, smallest, top_value):
    level, own = 1.0, jax.random.fold_in(key, 6)
    for axis_at, parts in cuts:
        steps = jnp.exp(jax.random.uniform(jax.random.fold_in(own, axis_at), (parts,), jnp.float32, smallest / len(cuts), top_value / len(cuts)))
        level = level * jnp.repeat(steps, extent[axis_at] // parts).reshape([-1 if axis == axis_at else 1 for axis in range(len(extent))])
    return level


def normal_values(own_key, dims, deviation, most, cuts=(), held_as=jnp.bfloat16):
    entries = deviation * jax.random.normal(own_key, dims, jnp.float32)
    if cuts:
        entries = entries * level_of(own_key, dims, cuts, -0.22, 0.18)
    return jnp.clip(entries, -most, most).astype(held_as)


def setup_inputs(seed: int = 0) -> dict:
    splits = jax.random.split(jax.random.key(seed), 9)
    tokens = normal_values(splits[0], (SEQS, LENGTH, D), 1.0, 6.0, ((0, 8), (1, 4)))
    up_weight = normal_values(splits[1], (D, WIDTH), D ** -0.5, 0.125, ((0, 8),))
    gate_weight = normal_values(splits[2], (D, WIDTH), D ** -0.5, 0.125, ((0, 8),))
    group_gain = jnp.clip(1.0 + 0.18 * jax.random.normal(splits[3], (GROUPS, GROUP_DIM), jnp.float32), 0.1, 1.9)
    mix_weight = normal_values(splits[4], (GROUPS, SPAN, SPAN), SPAN ** -0.5, 0.15625, ((0, 4), (1, 8)))
    mix_bias = jnp.clip(0.5 + 1.0 * jax.random.uniform(splits[5], (GROUPS, SPAN), jnp.float32) ** level_of(splits[5], (GROUPS, SPAN), ((0, 4),), -0.2, 0.2), 0.5, 1.5)
    out_gain = jnp.clip(1.0 + 0.18 * jax.random.normal(splits[6], (WIDTH,), jnp.float32), 0.1, 1.9)
    out_weight = normal_values(splits[7], (WIDTH, D), WIDTH ** -0.5, 0.125, ((1, 8),))
    return {"tokens": tokens, "up_weight": up_weight, "gate_weight": gate_weight, "group_gain": group_gain, "mix_weight": mix_weight, "mix_bias": mix_bias, "out_gain": out_gain, "out_weight": out_weight}


norm_eps = 1e-06

def reference(tokens, up_weight, gate_weight, group_gain, mix_weight, mix_bias, out_gain, out_weight):
    lower = jnp.tril(jnp.ones((SPAN, SPAN), dtype=bool))
    mix_mask = jnp.where(lower[None], mix_weight, jnp.zeros_like(mix_weight)).astype(jnp.float32)
    bias_cols = mix_bias.astype(jnp.float32).T

    def one_sequence(sequence):
        up_proj = jnp.dot(sequence, up_weight, preferred_element_type=jnp.float32).astype(jnp.bfloat16)
        gate_proj = jnp.dot(sequence, gate_weight, preferred_element_type=jnp.float32).astype(jnp.bfloat16)
        up_proj = lax.optimization_barrier(up_proj)
        gate_proj = lax.optimization_barrier(gate_proj)
        opened = jax.nn.gelu(up_proj.astype(jnp.float32)).reshape(LENGTH, GROUPS, GROUP_DIM)
        gate_act = jax.nn.gelu(gate_proj.astype(jnp.float32)).reshape(LENGTH, GROUPS, GROUP_DIM)
        center = lax.optimization_barrier(jnp.mean(gate_act, axis=-1, keepdims=True))
        spread = lax.optimization_barrier(jnp.mean(jnp.square(gate_act - center), axis=-1, keepdims=True))
        normal_v = ((gate_act - center) * lax.rsqrt(spread + norm_eps) * group_gain.astype(jnp.float32)).astype(jnp.bfloat16)
        normal_v = lax.optimization_barrier(normal_v)
        blocks = normal_v.astype(jnp.float32).reshape(LENGTH // SPAN, SPAN, GROUPS, GROUP_DIM)
        mixed_sum = jnp.einsum('gij,njgc->nigc', mix_mask, blocks) + bias_cols[None, :, :, None]
        gated = (opened * mixed_sum.reshape(LENGTH, GROUPS, GROUP_DIM)).astype(jnp.bfloat16)
        gated = lax.optimization_barrier(gated)
        gated_f = gated.astype(jnp.float32).reshape(LENGTH, WIDTH)
        scale = lax.rsqrt(lax.optimization_barrier(jnp.mean(gated_f * gated_f, axis=-1, keepdims=True)) + norm_eps)
        normed = (gated_f * scale * out_gain.astype(jnp.float32)).astype(jnp.bfloat16)
        return jnp.dot(normed, out_weight, preferred_element_type=jnp.float32).astype(jnp.bfloat16)
    return lax.map(one_sequence, tokens)
```

```python
import functools

import jax
import jax.numpy as jnp
from jax import lax
from jax.experimental import pallas as pl
from jax.experimental.pallas import tpu as pltpu
from jax.sharding import PartitionSpec as P

norm_eps = 1e-06
CORES = 2
LANES = 128
MESH = pl.DeviceIdType.MESH


def up_to(n, m):
    return -(-n // m) * m


def fused_kernel(
    sp, zs,
    tok_ref, up_ref, gate_ref, gain_ref, mix_ref, bias_ref, ogain_ref, outw_ref, out_ref,
    tok_v, ug_v, mix_v, outw_v, open_v, norm_v, other_v, bias_v, mixed_v, gated_v, held_v,
    normed_v, sums_v, part_v,
    load_sem,
    ug_line, ug_up, ug_dn, ug_ps, ug_pr,
    ow_line, ow_up, ow_dn, ow_ps, ow_pr, pl_s, pl_r, pp_s, pp_r,
    mx_line, mx_up, mx_dn, mx_ps, mx_pr,
    tok_s, tok_r, v_s, v_r, ret_s, ret_r, ga_s, ga_r,
):
    me = lax.axis_index("sp")
    dp = lax.axis_index("dp")
    z, c = dp // CORES, lax.rem(dp, CORES)
    groups, dps, rows, block = mix_v.shape
    per, width = out_ref.shape
    gd = gain_ref.shape[2]
    chans = groups * gd
    depth, ncol = up_ref.shape[0], outw_ref.shape[1]
    total = sp * per
    blocks = total // block
    parts, _, pk, _ = outw_v.shape
    zr = CORES * rows
    half, dhalf = per // 2, depth // 2
    square = sp == 4

    partner = {"dp": z * CORES + (1 - c)}

    def at_line(zz):
        return {"dp": zz * CORES + c}

    def around(r, sign):
        if square:
            y = lax.rem(me // 2 + r // 2, 2)
            x = lax.rem(lax.rem(me, 2) + r % 2, 2)
            return y * 2 + x
        return lax.rem(me + sign * r + sp, sp)

    def target(r):
        return around(r, 1)

    def source(r):
        return around(r, -1)

    def peer(r):
        return {"sp": target(r)}

    def inner(zz):
        return 0 < zz < zs - 1

    def mate(zz):
        return {0: 1, 1: 0, zs - 1: zs - 2, zs - 2: zs - 1}.get(zz)

    def remote(src, dst, send, recv, device):
        return pltpu.make_async_remote_copy(
            src_ref=src, dst_ref=dst, send_sem=send, recv_sem=recv,
            device_id=device, device_id_type=MESH)

    def arrived(ref, sem):
        remote(ref, ref, sem, sem, partner).wait_recv()

    def each_z(fn, only=None):
        for zz in range(zs):
            if only is None or only(zz):
                pl.when(z == zz)(functools.partial(fn, zz))

    def each_d(fn, only=None):
        for zz in range(zs):
            if only is None or only(zz):
                for cc in range(CORES):
                    pl.when(dp == zz * CORES + cc)(functools.partial(fn, zz, cc))

    loads = {"ug": [], "tok": [], "ow": [], "mx": []}
    for g in range(groups):
        for t, ref in enumerate((up_ref, gate_ref)):
            cols = pl.ds(pl.multiple_of(me * chans + g * gd, LANES), gd)
            spot = 2 * g + t
            loads["ug"].append(pltpu.make_async_copy(
                ref.at[:, cols],
                ug_v.at[pl.ds(dp * depth, depth), pl.ds(spot * gd, gd)],
                load_sem.at[3 + spot]))
    loads["tok"].append(pltpu.make_async_copy(tok_ref, tok_v.at[me], load_sem.at[0]))
    for p in range(parts):
        loads["ow"].append(pltpu.make_async_copy(
            outw_ref.at[pl.ds(me * chans + p * pk, pk), :],
            outw_v.at[p, me, :, pl.ds(pl.multiple_of(dp * ncol, LANES), ncol)],
            load_sem.at[3 + 2 * groups + p]))
    loads["mx"].append(pltpu.make_async_copy(mix_ref, mix_v.at[:, dp], load_sem.at[2]))
    for kind in ("ug", "tok", "ow", "mx"):
        for load in loads[kind]:
            load.start()

    barrier = pltpu.get_barrier_semaphore()

    def greet(zz):
        friends = [partner] + [peer(r) for r in range(1, sp)]
        if zz > 0:
            friends.append(at_line(zz - 1))
        if zz < zs - 1:
            friends.append(at_line(zz + 1))
        for friend in friends:
            pl.semaphore_signal(barrier, inc=1, device_id=friend, device_id_type=MESH)
        pl.semaphore_wait(barrier, len(friends))

    each_z(greet)

    def ug_piece(o, cc, h):
        return ug_v.at[pl.ds((o * CORES + cc) * depth + h * dhalf, dhalf), :]

    def ow_piece(s, o, cc):
        cols = pl.ds(pl.multiple_of((o * CORES + cc) * ncol, LANES), ncol)
        return outw_v.at[:, s, :, cols]

    def cuts(d):
        out, at, end = [], d * rows, (d + 1) * rows
        while at < end:
            top = min(end, (at // LANES + 1) * LANES)
            out.append((at - d * rows, top - at, min(block, up_to(top, LANES))))
            at = top
        return out

    def mx_piece(g, d, piece):
        r0, rn, cols = piece
        return mix_v.at[g, d, pl.ds(r0, rn), pl.ds(0, cols)]

    def ug_copies(zz, o, h):
        src, out = ug_piece(o, c, h), []
        if o >= zz and zz > 0:
            out.append(remote(src, src, ug_dn.at[o, h], ug_line.at[o, h], at_line(zz - 1)))
        if o <= zz and zz < zs - 1:
            out.append(remote(src, src, ug_up.at[o, h], ug_line.at[o, h], at_line(zz + 1)))
        out.append(remote(src, src, ug_ps.at[o, h], ug_pr.at[o, h], partner))
        return out

    def ow_down(zz, o):
        src = ow_piece(me, o, c)
        if o >= zz and zz > 0:
            return [remote(src, src, ow_dn.at[o], ow_line.at[o], at_line(zz - 1))]
        return []

    def ow_rise(zz, o):
        src = ow_piece(me, o, c)
        if o <= zz and zz < zs - 1:
            return [remote(src, src, ow_up.at[o], ow_line.at[o], at_line(zz + 1))]
        return []

    def ow_pair(o):
        src = ow_piece(me, o, c)
        return [remote(src, src, ow_ps.at[o], ow_pr.at[o], partner)]

    def mx_copies(zz, cc, g, o, way):
        out = []
        d = o * CORES + cc
        for i, piece in enumerate(cuts(d)):
            src = mx_piece(g, d, piece)
            if way == "dn" and o >= zz and inner(zz - 1):
                out.append(remote(src, src, mx_dn.at[g, o, i], mx_line.at[g, o, i], at_line(zz - 1)))
            if way == "up" and o <= zz and inner(zz + 1):
                out.append(remote(src, src, mx_up.at[g, o, i], mx_line.at[g, o, i], at_line(zz + 1)))
            if way == "pair" and (inner(zz) or o == zz):
                out.append(remote(src, src, mx_ps.at[g, o, i], mx_pr.at[g, o, i], partner))
        return out

    def go(copies):
        for copy in copies:
            copy.start()

    def own_mix(zz, way, low=0, high=groups):
        for cc in range(CORES):
            @pl.when(c == cc)
            def _():
                @pl.loop(low, high)
                def _(g):
                    go(mx_copies(zz, cc, g, zz, way))

    def ug_left(zz, way, k):
        far = zs - 1 - zz if way == "dn" else zz
        there = zz > 0 if way == "dn" else zz < zs - 1
        return there, max(0, far - k)

    held_back = max(1, groups - 1)

    def own_out(zz, way):
        go(ow_down(zz, zz) if way == "dn" else ow_rise(zz, zz))

    for load in loads["ug"]:
        load.wait()

    def first_weights(zz):
        for h in range(2):
            go(ug_copies(zz, zz, h))

    each_z(first_weights)
    for load in loads["tok"]:
        load.wait()

    def tok_half(s, h):
        return tok_v.at[s, pl.ds(h * half, half), :]

    def tok_copy(s, r, h, r_there):
        return remote(tok_half(s, h), tok_half(s, h), tok_s.at[r_there, h], tok_r.at[r_there, h], peer(r))

    def tok_first():
        if square:
            return [tok_copy(me, 1, 0, 1), tok_copy(me, 2, 1, 2), tok_copy(me, 1, 1, 1), tok_copy(me, 2, 0, 2)]
        return [tok_copy(me, r, h, r) for r in range(1, sp) for h in range(2)]

    def tok_second():
        if square:
            return [tok_copy(source(1), 2, 0, 3), tok_copy(source(2), 1, 1, 3)]
        return []

    go(tok_first())
    for load in loads["ow"] + loads["mx"]:
        load.wait()

    def first_rest(zz):
        go(ow_pair(zz))
        for way in ("dn", "up"):
            there, left = ug_left(zz, way, 0)
            if there and left == 0:
                own_out(zz, way)
                own_mix(zz, way, 0, held_back if zz == zs - 1 else groups)
        own_mix(zz, "pair")

    each_z(first_rest)

    for g in range(groups):
        for t in range(block // LANES):
            spot = slice(t * LANES, (t + 1) * LANES)
            bias_v[g, spot, :] = jnp.broadcast_to(bias_ref[g:g + 1, spot], (gd, LANES)).T

    def take_ug(zz, k):
        for o in (zz + k, zz - k):
            if 0 <= o < zs:
                for h in range(2):
                    arrived(ug_piece(o, c, h), ug_line.at[o, h])
                    go(ug_copies(zz, o, h))
        for way in ("dn", "up"):
            there, left = ug_left(zz, way, k)
            before = ug_left(zz, way, k - 1)[1]
            if there and left == 0 and before > 0:
                own_out(zz, way)
                own_mix(zz, way, 0, 1)

    def take_out(zz, k):
        for o in (zz + k, zz - k):
            if 0 <= o < zs:
                arrived(ow_piece(me, o, c), ow_line.at[o])
                go(ow_down(zz, o) if o > zz else ow_rise(zz, o))
                go(ow_pair(o))
        for way in ("dn", "up"):
            there, left = ug_left(zz, way, k)
            before = ug_left(zz, way, k - 1)[1]
            if there and left == 0 and before > 0:
                own_mix(zz, way, 1, groups)

    def plane_first(o):
        src = ow_piece(me, o, c)
        reach = (1, 2) if square else range(1, sp)
        return [remote(src, src, pl_s.at[r, o], pl_r.at[r, o], peer(r)) for r in reach]

    def plane_second(o):
        if not square:
            return []
        via, to = (1, 2) if o < zs // 2 else (2, 1)
        src = ow_piece(source(via), o, c)
        return [remote(src, src, pl_s.at[3, o], pl_r.at[3, o], peer(to))]

    def plane_pair(r, o):
        src = ow_piece(source(r), o, c)
        return [remote(src, src, pp_s.at[r, o], pp_r.at[r, o], partner)]

    each_z(lambda zz: take_ug(zz, 1))
    if square:
        arrived(tok_half(source(1), 0), tok_r.at[1, 0])
        arrived(tok_half(source(2), 1), tok_r.at[2, 1])
    go(tok_second())

    def more_weights(zz):
        for k in range(2, zs):
            take_ug(zz, k)
        if inner(zz) and not square:
            for k in range(1, zs):
                take_out(zz, k)
            for o in range(zs):
                go(plane_first(o))
        if not inner(zz):
            go(plane_first(zz))

    each_z(more_weights)

    def weights_in(zz):
        for o in range(zs):
            for h in range(2):
                arrived(ug_piece(o, 1 - c, h), ug_pr.at[o, h])

    weights_in(None)

    def v_copy(zz, q):
        spot = pl.ds(pl.multiple_of(q * per, 16), per)
        return remote(norm_v.at[:, spot, :], other_v.at[:, spot, :],
                      v_s.at[q], v_r.at[q], at_line(mate(zz)))

    def starts(q):
        return (q * per) % block

    def v_useful(end, q):
        return any(starts(q) < (o + 1) * zr for o in range(zs) if o != end) or block % per > 0

    def send_v(zz, s):
        for q in range(sp):
            if v_useful(zz, q):
                pl.when(s == q)(lambda q=q: v_copy(zz, q).start())

    def project(s):
        spot = pl.ds(pl.multiple_of(s * per, 16), per)

        @pl.loop(0, groups)
        def _(g):
            cols = pl.ds(pl.multiple_of(g * 2 * gd, 2 * gd), 2 * gd)
            both = jnp.dot(tok_v[s], ug_v[:, cols], preferred_element_type=jnp.float32)
            both = jax.nn.gelu(both.astype(jnp.bfloat16).astype(jnp.float32))
            open_v[g, spot, :] = both[:, :gd]
            act = both[:, gd:]
            act = act - jnp.mean(act, axis=-1, keepdims=True)
            spread = jnp.mean(act * act, axis=-1, keepdims=True)
            norm_v[g, spot, :] = (
                act * lax.rsqrt(spread + norm_eps) * gain_ref[g]
            ).astype(jnp.bfloat16)

        each_z(lambda zz: send_v(zz, s), lambda zz: not inner(zz))

    def out_events(zz, ks):
        for k in ks:
            take_out(zz, k)
            for o in (zz + k, zz - k):
                if 0 <= o < zs:
                    go(plane_first(o))
            if inner(zz) and k == 1:
                go(plane_first(zz))

    if square:
        for r in range(sp):
            for h in range(2 if r else 0):
                if r != 1 + h:
                    arrived(tok_half(source(r), h), tok_r.at[r, h])
            project(source(r))

            def events(zz, r=r):
                first = r + 1 if inner(zz) else r
                ks = range(first, zs if r == sp - 1 else first + 1)
                out_events(zz, [k for k in ks if 0 < k < zs])

            each_z(events)
    else:
        @pl.loop(0, sp)
        def _(r):
            @pl.when(r > 0)
            def _():
                for h in range(2):
                    arrived(tok_half(source(r), h), tok_r.at[r, h])

            project(source(r))

        each_z(lambda zz: out_events(zz, range(1, zs)), lambda zz: not inner(zz))

    if held_back < groups:
        each_z(lambda zz: own_mix(zz, "dn", held_back, groups), lambda zz: zz == zs - 1)

    def take_mix(zz, cc, g, o):
        d = o * CORES + cc
        for i, piece in enumerate(cuts(d)):
            arrived(mx_piece(g, d, piece), mx_line.at[g, o, i])
        go(mx_copies(zz, cc, g, o, "dn" if o > zz else "up"))
        go(mx_copies(zz, cc, g, o, "pair"))

    def passed_on(zz, o):
        return abs(o - zz) == 1 and inner(zz - 1 if o > zz else zz + 1)

    def late(zz, o):
        return zz == zs - 2 and o == zs - 1

    def near_mix(zz, cc):
        for o in (zz + 1, zz - 1):
            if passed_on(zz, o):
                @pl.loop(0, held_back if late(zz, o) else groups)
                def _(g):
                    take_mix(zz, cc, g, o)

    def late_mix(zz, cc):
        @pl.loop(held_back, groups)
        def _(g):
            take_mix(zz, cc, g, zz + 1)

    each_d(near_mix, inner)

    def ready_at(q):
        if block % per:
            return zs - 1
        return (((q + 1) * per - 1) % block) // zr

    def needs(o):
        return min(block, up_to((o + 1) * zr, LANES))

    def first_need(zz, q):
        if not v_useful(mate(zz), q):
            return None
        return next(o for o in range(zs) if o != mate(zz) and (block % per or starts(q) < needs(o)))

    def with_mate(zz, o):
        return inner(zz) and mate(zz) is not None and mate(zz) != o

    def alone(zz, o):
        return zz == o if not inner(zz) else not with_mate(zz, o)

    def gated_copy(g, q):
        return remote(gated_v.at[g, pl.ds(q * per, per), :], held_v.at[me, g],
                      ga_s.at[g, q], ga_r.at[g, me], {"sp": q})

    def ret_copy(zz, g, o):
        spot = mixed_v.at[g, :, o]
        return remote(spot, spot, ret_s.at[g, o], ret_r.at[g, o], at_line(mate(zz)))

    def hand_over(g, o):
        for q in range(sp):
            if ready_at(q) == o:
                @pl.when(me == q)
                def _():
                    held_v[q, g] = gated_v[g, pl.ds(q * per, per), :]

                @pl.when(me != q)
                def _():
                    gated_copy(g, q).start()

    def one_of(zs_in):
        return functools.reduce(jnp.logical_or, [z == zz for zz in zs_in])

    def clear_unsent(zz):
        for q in range(sp):
            if not v_useful(mate(zz), q):
                high = max(needs(o) for o in range(zs) if o != mate(zz)) - starts(q)
                if high > 0:
                    other_v[:, q * per:q * per + high, :] = jnp.zeros(
                        (groups, high, gd), jnp.bfloat16)

    each_z(clear_unsent, lambda zz: inner(zz) and mate(zz) is not None)

    def unit(o, low=0, high=groups, only=None, but=None):
        lo = o * zr
        base, top = lo // LANES * LANES, needs(o)

        def wait_v(zz):
            for q in range(sp):
                if first_need(zz, q) == o:
                    arrived(other_v.at[:, pl.ds(q * per, per), :], v_r.at[q])

        if low == 0:
            each_z(wait_v, lambda zz: with_mate(zz, o))

        def mix(members, paired):
            @pl.loop(low, high)
            def _(g):
                def rows_in(zz, cc):
                    if o != zz and not passed_on(zz, o):
                        take_mix(zz, cc, g, o)
                    d = o * CORES + 1 - cc
                    for i, piece in enumerate(cuts(d)):
                        arrived(mx_piece(g, d, piece), mx_pr.at[g, o, i])

                def values(at, end):
                    own = norm_v[g, at:end, :]
                    return jnp.concatenate([own, other_v[g, at:end, :]], axis=1) if paired else own

                each_d(rows_in, lambda zz: zz in members)
                corner = mix_v[g, o * CORES:(o + 1) * CORES, :, base:top].reshape(zr, top - base)
                keep = lax.broadcasted_iota(jnp.int32, corner.shape, 0) + (lo - base) >= (
                    lax.broadcasted_iota(jnp.int32, corner.shape, 1))
                corner = jnp.where(keep, corner.astype(jnp.float32), 0.0).astype(jnp.bfloat16)
                bias = bias_v[g, lo:lo + zr, :]
                for b in range(blocks):
                    at = b * block
                    mixed = jnp.dot(corner, values(at + base, at + top),
                                    preferred_element_type=jnp.float32)
                    if base > 0:
                        left = mix_v[g, o * CORES:(o + 1) * CORES, :, :base].reshape(zr, base)
                        mixed += jnp.dot(left, values(at, at + base),
                                         preferred_element_type=jnp.float32)
                    spot = slice(at + lo, at + lo + zr)
                    if paired:
                        mixed_v[g, b, o] = (mixed[:, gd:] + bias).astype(jnp.bfloat16)
                    gated_v[g, spot, :] = (
                        open_v[g, spot, :] * (mixed[:, :gd] + bias)).astype(jnp.bfloat16)
                if paired:
                    each_z(lambda zz: ret_copy(zz, g, o).start(), lambda zz: zz in members)
                hand_over(g, o)

        for paired, test in ((True, with_mate), (False, alone)):
            members = [zz for zz in range(zs) if test(zz, o) and zz != but and only in (None, zz)]
            if members:
                pl.when(one_of(members))(functools.partial(mix, members, paired))

        if only is not None:
            return

        @pl.when(one_of([zz for zz in (0, zs - 1) if zz != o]))
        def _():
            @pl.loop(low, high)
            def _(g):
                arrived(mixed_v.at[g, :, o], ret_r.at[g, o])
                for b in range(blocks):
                    spot = slice(b * block + lo, b * block + lo + zr)
                    gated_v[g, spot, :] = (
                        open_v[g, spot, :] * mixed_v[g, b, o].astype(jnp.float32)
                    ).astype(jnp.bfloat16)
                hand_over(g, o)

    for o in range(zs):
        for r in range(1, sp):
            if not (square and r == 3):
                arrived(ow_piece(source(r), o, c), pl_r.at[r, o])
        go(plane_second(o))
        for r in range(1, sp):
            if not (square and r == 3):
                go(plane_pair(r, o))

    unit(zs - 1, only=zs - 1)
    for o in range(zs - 1):
        unit(o)
        if o == 0 and held_back < groups:
            each_d(late_mix, lambda zz: late(zz, zz + 1))

    if square:
        for o in range(zs):
            arrived(ow_piece(source(3), o, c), pl_r.at[3, o])
            go(plane_pair(3, o))

    def gone(copies):
        for copy in copies:
            copy.wait_send()

    def line_gone(zz):
        for o in range(zs):
            for h in range(2):
                gone(ug_copies(zz, o, h))
            gone(ow_down(zz, o) + ow_rise(zz, o))
        if not inner(zz):
            gone([v_copy(zz, q) for q in range(sp) if v_useful(zz, q)])

    gone(tok_first() + tok_second())
    for o in range(zs):
        gone(plane_first(o) + ow_pair(o))
        for r in range(1, sp):
            if not (square and r == 3):
                gone(plane_pair(r, o))
    each_z(line_gone)

    per_part = groups // parts

    def gather_part(p):
        for s in range(sp):
            @pl.when(me != s)
            def _():
                for g in range(p * per_part, (p + 1) * per_part):
                    arrived(held_v.at[s, g], ga_r.at[g, s])
        squares = jnp.zeros((per, gd), jnp.float32)
        for s in range(sp):
            for i in range(per_part):
                g = p * per_part + i
                value = held_v[s, g].astype(jnp.float32)
                squares += value * value
                cols = slice(s * chans + g * gd, s * chans + (g + 1) * gd)
                normed_v[p, :, s * pk + i * gd:s * pk + (i + 1) * gd] = (
                    value * ogain_ref[:, cols]).astype(jnp.bfloat16)
        sums_v[...] = squares if p == 0 else sums_v[...] + squares

    def part_dot(p, cols):
        return jnp.dot(normed_v[p], outw_v[p, :, :, cols].reshape(sp * pk, ncol),
                       preferred_element_type=jnp.float32)

    def weights_here():
        for o in range(zs):
            arrived(ow_piece(me, o, 1 - c), ow_pr.at[o])
            for r in range(1, sp):
                arrived(ow_piece(source(r), o, 1 - c), pp_r.at[r, o])

    weights_here()
    if parts > 1:
        unit(zs - 1, 0, groups - 1, but=zs - 1)
        gather_part(0)

        @pl.loop(0, width // ncol)
        def _(t):
            cols = pl.ds(pl.multiple_of(t * ncol, LANES), ncol)
            part_v[:, cols] = part_dot(0, cols)

        unit(zs - 1, groups - 1, groups, but=zs - 1)
    else:
        unit(zs - 1, but=zs - 1)
    gather_part(parts - 1)
    scale = lax.rsqrt(jnp.sum(sums_v[...], axis=-1, keepdims=True) / (sp * chans) + norm_eps)

    @pl.loop(0, width // ncol)
    def _(t):
        cols = pl.ds(pl.multiple_of(t * ncol, LANES), ncol)
        last = part_dot(parts - 1, cols)
        if parts > 1:
            last += part_v[:, cols]
        out_ref[:, cols] = (last * scale).astype(jnp.bfloat16)

    for o in range(zs):
        gone(plane_second(o))
        if square:
            gone(plane_pair(3, o))

    def rest_gone(zz):
        @pl.loop(0, groups)
        def _(g):
            gone([ret_copy(zz, g, o) for o in range(zs) if with_mate(zz, o)])

    each_z(rest_gone, lambda zz: inner(zz) and mate(zz) is not None)

    def mix_gone(zz, cc):
        @pl.loop(0, groups)
        def _(g):
            for o in range(zs):
                if o == zz:
                    ways = ("dn", "up", "pair")
                elif inner(zz):
                    ways = ("dn" if o > zz else "up", "pair")
                else:
                    ways = ()
                for way in ways:
                    gone(mx_copies(zz, cc, g, o, way))

    each_d(mix_gone)
    for q in range(sp):
        @pl.when(me != q)
        def _():
            @pl.loop(0, groups)
            def _(g):
                gone([gated_copy(g, q)])


def body(tokens, up_weight, gate_weight, group_gain, mix_weight, mix_bias, out_gain, out_weight):
    per, width = tokens.shape[1:]
    groups, gd = group_gain.shape
    rows, block = mix_weight.shape[1:]
    sp, dps = lax.axis_size("sp"), lax.axis_size("dp")
    zs = dps // CORES
    total = sp * per
    parts = 1 if groups % 2 else 2
    bf, f32 = jnp.bfloat16, jnp.float32
    dma = pltpu.SemaphoreType.DMA
    hbm = pl.BlockSpec(memory_space=pltpu.HBM)
    vmem = pl.BlockSpec(memory_space=pltpu.VMEM)
    output = pl.pallas_call(
        functools.partial(fused_kernel, sp, zs),
        out_shape=pltpu.VMEM((per, width), bf),
        in_specs=[hbm, hbm, hbm, vmem, hbm, vmem, vmem, hbm],
        out_specs=vmem,
        scratch_shapes=[
            pltpu.VMEM((sp, per, width), bf),
            pltpu.VMEM((width, 2 * groups * gd), bf),
            pltpu.VMEM((groups, dps, rows, block), bf),
            pltpu.VMEM((parts, sp, groups * gd // parts, width), bf),
            pltpu.VMEM((groups, total, gd), f32),
            pltpu.VMEM((groups, total, gd), bf),
            pltpu.VMEM((groups, total, gd), bf),
            pltpu.VMEM((groups, block, gd), f32),
            pltpu.VMEM((groups, total // block, zs, CORES * rows, gd), bf),
            pltpu.VMEM((groups, total, gd), bf),
            pltpu.VMEM((sp, groups, per, gd), bf),
            pltpu.VMEM((parts, per, sp * groups * gd // parts), bf),
            pltpu.VMEM((per, gd), f32),
            pltpu.VMEM((per, width if parts > 1 else gd), f32),
            dma((3 + 2 * groups + parts,)),
        ] + [dma((zs, 2))] * 5 + [dma((zs,))] * 5 + [dma((sp, zs))] * 4
        + [dma((groups, zs, 2))] * 5 + [dma((sp, 2))] * 2 + [dma((sp,))] * 2
        + [dma((groups, zs))] * 2 + [dma((groups, sp))] * 2,
        compiler_params=pltpu.CompilerParams(collective_id=0, has_side_effects=True, vmem_limit_bytes=65_000_000),
    )(tokens.reshape(per, width), up_weight, gate_weight, group_gain[:, None, :], mix_weight, mix_bias,
      out_gain[None, :], out_weight)
    return output.reshape(tokens.shape)


def solution(mesh):
    return jax.shard_map(
        body,
        mesh=mesh,
        in_specs=(
            P("dp", "sp", None),
            P("dp", None),
            P("dp", None),
            P("sp", None),
            P("sp", "dp", None),
            P("sp", None),
            P(),
            P(None, "dp"),
        ),
        out_specs=P("dp", "sp", None),
        check_vma=False,
    )
```

```python
import functools

import jax
import jax.numpy as jnp
from jax import lax
from jax.experimental import pallas as pl
from jax.experimental.pallas import tpu as pltpu
from jax.sharding import PartitionSpec as P

norm_eps = 1e-06
CORES = 2
LANES = 128
MESH = pl.DeviceIdType.MESH


def up_to(n, m):
    return -(-n // m) * m


def fused_kernel(
    sp, zs,
    tok_ref, up_ref, gate_ref, gain_ref, mix_ref, bias_ref, ogain_ref, outw_ref, out_ref,
    tok_v, ug_v, mix_v, outw_v, open_v, norm_v, other_v, bias_v, mixed_v, gated_v, held_v,
    normed_v, sums_v, part_v,
    load_sem, ug_line, ug_send, ug_pr, ow_line, ow_send, ow_pr, ow_own,
    pl_s, pl_r, p2_s, p2_r, pp_s, pp_r, mx_line, mx_pr, mx_up, mx_dn, mx_ps,
    tok_s, tok_r, v_s, v_r, ret_s, ret_r, ga_s, ga_r,
):
    me = lax.axis_index("sp")
    dp = lax.axis_index("dp")
    z, c = dp // CORES, lax.rem(dp, CORES)
    groups, dps, rows, block = mix_v.shape
    per, width = out_ref.shape
    gd = gain_ref.shape[2]
    chans = groups * gd
    depth, ncol = up_ref.shape[0], outw_ref.shape[3]
    total = sp * per
    blocks = total // block
    per_part = groups // outw_v.shape[0]
    parts, _, pk, _ = outw_v.shape
    zr = CORES * rows
    half, dhalf = per // 2, depth // 2
    square = sp == 4

    partner = {"dp": z * CORES + (1 - c)}

    def at_line(zz):
        return {"dp": zz * CORES + c}

    def around(r, sign):
        if square:
            y = lax.rem(me // 2 + r // 2, 2)
            x = lax.rem(lax.rem(me, 2) + r % 2, 2)
            return y * 2 + x
        return lax.rem(me + sign * r + sp, sp)

    def target(r):
        return around(r, 1)

    def source(r):
        return around(r, -1)

    def peer(r):
        return {"sp": target(r)}

    def inner(zz):
        return 0 < zz < zs - 1

    def mate(zz):
        return {0: 1, 1: 0, zs - 1: zs - 2, zs - 2: zs - 1}.get(zz)

    def remote(src, dst, send, recv, device):
        return pltpu.make_async_remote_copy(
            src_ref=src, dst_ref=dst, send_sem=send, recv_sem=recv,
            device_id=device, device_id_type=MESH)

    def sent(ref, sem):
        remote(ref, ref, sem, sem, partner).wait_send()

    def arrived(ref, sem):
        remote(ref, ref, sem, sem, partner).wait_recv()

    def each_z(fn, only=None):
        for zz in range(zs):
            if only is None or only(zz):
                pl.when(z == zz)(functools.partial(fn, zz))

    def each_d(fn, only=None):
        for zz in range(zs):
            if only is None or only(zz):
                for cc in range(CORES):
                    pl.when(dp == zz * CORES + cc)(functools.partial(fn, zz, cc))

    loads = {"ug": [], "tok": [], "ow": [], "mx": []}
    for g in range(groups):
        for t, ref in enumerate((up_ref, gate_ref)):
            cols = pl.ds(pl.multiple_of(me * chans + g * gd, LANES), gd)
            spot = 2 * g + t
            loads["ug"].append(pltpu.make_async_copy(
                ref.at[:, cols],
                ug_v.at[pl.ds(dp * depth, depth), pl.ds(spot * gd, gd)],
                load_sem.at[3]))
    loads["tok"].append(pltpu.make_async_copy(tok_ref, tok_v.at[me], load_sem.at[0]))
    own_cols = pl.ds(pl.multiple_of(dp * ncol, LANES), ncol)
    for p in range(parts):
        loads["ow"].append(pltpu.make_async_copy(
            outw_ref.at[:, p], outw_v.at[p, :, :, own_cols], load_sem.at[1]))
    loads["mx"].append(pltpu.make_async_copy(mix_ref, mix_v.at[:, dp], load_sem.at[2]))
    for kind in ("ug", "tok", "ow", "mx"):
        for load in loads[kind]:
            load.start()

    def loaded(ref, sem):
        pltpu.make_async_copy(ref, ref, sem).wait()

    barrier = pltpu.get_barrier_semaphore()

    def greet(zz):
        friends = [partner] + [peer(r) for r in range(1, sp)]
        if zz > 0:
            friends.append(at_line(zz - 1))
        if zz < zs - 1:
            friends.append(at_line(zz + 1))
        for friend in friends:
            pl.semaphore_signal(barrier, inc=1, device_id=friend, device_id_type=MESH)
        pl.semaphore_wait(barrier, len(friends))

    each_z(greet)

    def ug_piece(o, cc, h):
        return ug_v.at[pl.ds((o * CORES + cc) * depth + h * dhalf, dhalf), :]

    def ow_piece(s, o, cc):
        cols = pl.ds(pl.multiple_of((o * CORES + cc) * ncol, LANES), ncol)
        return outw_v.at[:, s, :, cols]

    def cuts(d):
        out, at, end = [], d * rows, (d + 1) * rows
        while at < end:
            top = min(end, (at // LANES + 1) * LANES)
            out.append((at - d * rows, top - at, min(block, up_to(top, LANES))))
            at = top
        return out

    def mx_piece(g, d, piece):
        r0, rn, cols = piece
        return mix_v.at[g, d, pl.ds(r0, rn), pl.ds(0, cols)]

    def ug_copies(zz, o, h):
        src, out = ug_piece(o, c, h), []
        if o >= zz and zz > 0:
            out.append(remote(src, src, ug_send.at[1], ug_line.at[o, h], at_line(zz - 1)))
        if o <= zz and zz < zs - 1:
            out.append(remote(src, src, ug_send.at[0], ug_line.at[o, h], at_line(zz + 1)))
        out.append(remote(src, src, ug_send.at[2], ug_pr.at[0], partner))
        return out

    def ow_down(zz, o):
        src = ow_piece(me, o, c)
        if o >= zz and zz > 0:
            return [remote(src, src, ow_send.at[1], ow_line.at[o], at_line(zz - 1))]
        return []

    def ow_rise(zz, o):
        src = ow_piece(me, o, c)
        if o <= zz and zz < zs - 1:
            return [remote(src, src, ow_send.at[0], ow_line.at[o], at_line(zz + 1))]
        return []

    def ow_pair(o):
        src = ow_piece(me, o, c)
        return [remote(src, src, ow_send.at[2], ow_pr.at[0], partner)]

    def ow_own_pair():
        src = outw_v.at[:, :, :, own_cols]
        return [remote(src, src, ow_own.at[0], ow_own.at[1], partner)]

    def ow_bytes(n):
        return outw_v.at[:, 0, :, pl.ds(0, n * ncol)]

    def mx_copies(zz, cc, g, o, way):
        out = []
        d = o * CORES + cc
        for i, piece in enumerate(cuts(d)):
            src = mx_piece(g, d, piece)
            if way == "dn" and o >= zz and inner(zz - 1):
                out.append(remote(src, src, mx_dn.at[o, i], mx_line.at[g, o, i], at_line(zz - 1)))
            if way == "up" and o <= zz and inner(zz + 1):
                out.append(remote(src, src, mx_up.at[o, i], mx_line.at[g, o, i], at_line(zz + 1)))
            if way == "pair" and (inner(zz) or o == zz):
                out.append(remote(src, src, mx_ps.at[o, i], mx_pr.at[g, o, i], partner))
        return out

    def go(copies):
        for copy in copies:
            copy.start()

    def own_mix(zz, way, low=0, high=groups):
        for cc in range(CORES):
            @pl.when(c == cc)
            def _():
                @pl.loop(low, high)
                def _(g):
                    go(mx_copies(zz, cc, g, zz, way))

    def ug_left(zz, way, k):
        far = zs - 1 - zz if way == "dn" else zz
        there = zz > 0 if way == "dn" else zz < zs - 1
        return there, max(0, far - k)

    held_back = max(1, groups - 1)

    def own_out(zz, way):
        go(ow_down(zz, zz) if way == "dn" else ow_rise(zz, zz))

    loaded(ug_v.at[pl.ds(dp * depth, depth), :], load_sem.at[3])

    def first_weights(zz):
        for h in range(2):
            go(ug_copies(zz, zz, h))

    each_z(first_weights)
    for load in loads["tok"]:
        load.wait()

    def tok_half(s, h):
        return tok_v.at[s, pl.ds(h * half, half), :]

    def tok_copy(s, r, h, r_there):
        return remote(tok_half(s, h), tok_half(s, h), tok_s.at[0], tok_r.at[r_there, h], peer(r))

    def tok_first():
        if square:
            return [tok_copy(me, 1, 0, 1), tok_copy(me, 2, 1, 2), tok_copy(me, 1, 1, 1), tok_copy(me, 2, 0, 2)]
        return [tok_copy(me, r, h, r) for r in range(1, sp) for h in range(2)]

    def tok_second():
        if square:
            return [tok_copy(source(1), 2, 0, 3), tok_copy(source(2), 1, 1, 3)]
        return []

    go(tok_first())
    loaded(outw_v.at[:, :, :, own_cols], load_sem.at[1])
    loads["mx"][0].wait()
    go(ow_own_pair())

    def first_rest(zz):
        for way in ("dn", "up"):
            there, left = ug_left(zz, way, 0)
            if there and left == 0:
                own_out(zz, way)
                own_mix(zz, way, 0, held_back if zz == zs - 1 else groups)
        own_mix(zz, "pair")

    each_z(first_rest)

    for g in range(groups):
        for t in range(block // LANES):
            spot = slice(t * LANES, (t + 1) * LANES)
            bias_v[g, spot, :] = jnp.broadcast_to(bias_ref[g:g + 1, spot], (gd, LANES)).T

    def take_ug(zz, k):
        for o in (zz + k, zz - k):
            if 0 <= o < zs:
                for h in range(2):
                    arrived(ug_piece(o, c, h), ug_line.at[o, h])
                    go(ug_copies(zz, o, h))
        for way in ("dn", "up"):
            there, left = ug_left(zz, way, k)
            before = ug_left(zz, way, k - 1)[1]
            if there and left == 0 and before > 0:
                own_out(zz, way)
                own_mix(zz, way, 0, 1)

    def take_out(zz, k):
        for o in (zz + k, zz - k):
            if 0 <= o < zs:
                arrived(ow_piece(me, o, c), ow_line.at[o])
                go(ow_down(zz, o) if o > zz else ow_rise(zz, o))
                go(ow_pair(o))
        for way in ("dn", "up"):
            there, left = ug_left(zz, way, k)
            before = ug_left(zz, way, k - 1)[1]
            if there and left == 0 and before > 0:
                own_mix(zz, way, 1, groups)

    def others(zz):
        return [o for k in range(1, zs) for o in (zz + k, zz - k) if 0 <= o < zs]

    def plane_first(o):
        src = ow_piece(me, o, c)
        reach = (1, 2) if square else range(1, sp)
        return [remote(src, src, pl_s.at[r], pl_r.at[r, o], peer(r)) for r in reach]

    def second_part(s, o, p):
        cols = pl.ds(pl.multiple_of((o * CORES + c) * ncol, LANES), ncol)
        return outw_v.at[p, s, :, cols]

    def plane_second(zz, o):
        if not square:
            return []
        units = [(x, p) for x in others(zz) for p in range(parts)]
        out = []
        for p in range(parts):
            via, to = (1, 2) if units.index((o, p)) < len(units) // 2 else (2, 1)
            src = second_part(source(via), o, p)
            out.append(remote(src, src, p2_s.at[0], p2_r.at[o, p], peer(to)))
        return out

    def plane_pair(r, o):
        src = ow_piece(source(r), o, c)
        return [remote(src, src, pp_s.at[r], pp_r.at[r], partner)]

    each_z(lambda zz: take_ug(zz, 1))
    if square:
        arrived(tok_half(source(1), 0), tok_r.at[1, 0])
        arrived(tok_half(source(2), 1), tok_r.at[2, 1])
    go(tok_second())

    def more_weights(zz):
        for k in range(2, zs):
            take_ug(zz, k)
        if inner(zz) and not square:
            for k in range(1, zs):
                take_out(zz, k)
            for o in others(zz):
                go(plane_first(o))

    each_z(more_weights)

    arrived(ug_v.at[pl.ds(0, zs * depth), :], ug_pr.at[0])

    def v_copy(zz, q):
        spot = pl.ds(pl.multiple_of(q * per, 16), per)
        return remote(norm_v.at[:, spot, :], other_v.at[:, spot, :],
                      v_s.at[0], v_r.at[q], at_line(mate(zz)))

    def starts(q):
        return (q * per) % block

    def v_useful(end, q):
        return any(starts(q) < (o + 1) * zr for o in range(zs) if o != end) or block % per > 0

    def send_v(zz, s):
        for q in range(sp):
            if v_useful(zz, q):
                pl.when(s == q)(lambda q=q: v_copy(zz, q).start())

    def project(s):
        spot = pl.ds(pl.multiple_of(s * per, 16), per)

        @pl.loop(0, groups)
        def _(g):
            cols = pl.ds(pl.multiple_of(g * 2 * gd, 2 * gd), 2 * gd)
            both = jnp.dot(tok_v[s], ug_v[:, cols], preferred_element_type=jnp.float32)
            both = jax.nn.gelu(both.astype(jnp.bfloat16).astype(jnp.float32))
            open_v[g, spot, :] = both[:, :gd]
            act = both[:, gd:]
            act = act - jnp.mean(act, axis=-1, keepdims=True)
            spread = jnp.mean(act * act, axis=-1, keepdims=True)
            norm_v[g, spot, :] = (
                act * lax.rsqrt(spread + norm_eps) * gain_ref[g]
            ).astype(jnp.bfloat16)

        each_z(lambda zz: send_v(zz, s), lambda zz: not inner(zz))

    def out_events(zz, ks):
        for k in ks:
            take_out(zz, k)
            for o in (zz + k, zz - k):
                if 0 <= o < zs:
                    go(plane_first(o))

    if square:
        for r in range(sp):
            for h in range(2 if r else 0):
                if r != 1 + h:
                    arrived(tok_half(source(r), h), tok_r.at[r, h])
            project(source(r))

            def events(zz, r=r):
                first = r + 1 if inner(zz) else r
                ks = range(first, zs if r == sp - 1 else first + 1)
                out_events(zz, [k for k in ks if 0 < k < zs])

            each_z(events)
    else:
        @pl.loop(0, sp)
        def _(r):
            @pl.when(r > 0)
            def _():
                for h in range(2):
                    arrived(tok_half(source(r), h), tok_r.at[r, h])

            project(source(r))

        each_z(lambda zz: out_events(zz, range(1, zs)), lambda zz: not inner(zz))

    if held_back < groups:
        each_z(lambda zz: own_mix(zz, "dn", held_back, groups), lambda zz: zz == zs - 1)

    def take_mix(zz, cc, g, o):
        d = o * CORES + cc
        for i, piece in enumerate(cuts(d)):
            arrived(mx_piece(g, d, piece), mx_line.at[g, o, i])
        go(mx_copies(zz, cc, g, o, "dn" if o > zz else "up"))
        go(mx_copies(zz, cc, g, o, "pair"))

    def passed_on(zz, o):
        return abs(o - zz) == 1 and inner(zz - 1 if o > zz else zz + 1)

    def late(zz, o):
        return zz == zs - 2 and o == zs - 1

    def near_mix(zz, cc):
        for o in (zz + 1, zz - 1):
            if passed_on(zz, o):
                @pl.loop(0, held_back if late(zz, o) else groups)
                def _(g):
                    take_mix(zz, cc, g, o)

    def late_mix(zz, cc):
        @pl.loop(held_back, groups)
        def _(g):
            take_mix(zz, cc, g, zz + 1)

    each_d(near_mix, inner)

    def ready_at(q):
        if block % per:
            return zs - 1
        return (((q + 1) * per - 1) % block) // zr

    def needs(o):
        return min(block, up_to((o + 1) * zr, LANES))

    def first_need(zz, q):
        if not v_useful(mate(zz), q):
            return None
        return next(o for o in range(zs) if o != mate(zz) and (block % per or starts(q) < needs(o)))

    def with_mate(zz, o):
        return inner(zz) and mate(zz) is not None and mate(zz) != o

    def alone(zz, o):
        return zz == o if not inner(zz) else not with_mate(zz, o)

    def gated_copy(g, q):
        return remote(gated_v.at[g, pl.ds(q * per, per), :], held_v.at[me, g],
                      ga_s.at[0], ga_r.at[g // per_part, me], {"sp": q})

    def ret_copy(zz, g, o):
        spot = mixed_v.at[g, :, o]
        return remote(spot, spot, ret_s.at[0], ret_r.at[g, o], at_line(mate(zz)))

    def hand_over(g, o):
        for q in range(sp):
            if ready_at(q) == o:
                @pl.when(me == q)
                def _():
                    held_v[q, g] = gated_v[g, pl.ds(q * per, per), :]

                @pl.when(me != q)
                def _():
                    gated_copy(g, q).start()

    def one_of(zs_in):
        return functools.reduce(jnp.logical_or, [z == zz for zz in zs_in])

    def clear_unsent(zz):
        for q in range(sp):
            if not v_useful(mate(zz), q):
                high = max(needs(o) for o in range(zs) if o != mate(zz)) - starts(q)
                if high > 0:
                    other_v[:, q * per:q * per + high, :] = jnp.zeros(
                        (groups, high, gd), jnp.bfloat16)

    each_z(clear_unsent, lambda zz: inner(zz) and mate(zz) is not None)

    def unit(o, low=0, high=groups, only=None, but=None):
        lo = o * zr
        base, top = lo // LANES * LANES, needs(o)

        def wait_v(zz):
            for q in range(sp):
                if first_need(zz, q) == o:
                    arrived(other_v.at[:, pl.ds(q * per, per), :], v_r.at[q])

        if low == 0:
            each_z(wait_v, lambda zz: with_mate(zz, o))

        def mix(members, paired):
            @pl.loop(low, high)
            def _(g):
                def rows_in(zz, cc):
                    if o != zz and not passed_on(zz, o):
                        take_mix(zz, cc, g, o)
                    d = o * CORES + 1 - cc
                    for i, piece in enumerate(cuts(d)):
                        arrived(mx_piece(g, d, piece), mx_pr.at[g, o, i])

                def values(at, end):
                    own = norm_v[g, at:end, :]
                    return jnp.concatenate([own, other_v[g, at:end, :]], axis=1) if paired else own

                each_d(rows_in, lambda zz: zz in members)
                corner = mix_v[g, o * CORES:(o + 1) * CORES, :, base:top].reshape(zr, top - base)
                keep = lax.broadcasted_iota(jnp.int32, corner.shape, 0) + (lo - base) >= (
                    lax.broadcasted_iota(jnp.int32, corner.shape, 1))
                corner = jnp.where(keep, corner.astype(jnp.float32), 0.0).astype(jnp.bfloat16)
                bias = bias_v[g, lo:lo + zr, :]
                for b in range(blocks):
                    at = b * block
                    mixed = jnp.dot(corner, values(at + base, at + top),
                                    preferred_element_type=jnp.float32)
                    if base > 0:
                        left = mix_v[g, o * CORES:(o + 1) * CORES, :, :base].reshape(zr, base)
                        mixed += jnp.dot(left, values(at, at + base),
                                         preferred_element_type=jnp.float32)
                    spot = slice(at + lo, at + lo + zr)
                    if paired:
                        mixed_v[g, b, o] = (mixed[:, gd:] + bias).astype(jnp.bfloat16)
                    gated_v[g, spot, :] = (
                        open_v[g, spot, :] * (mixed[:, :gd] + bias)).astype(jnp.bfloat16)
                if paired:
                    each_z(lambda zz: ret_copy(zz, g, o).start(), lambda zz: zz in members)
                hand_over(g, o)

        for paired, test in ((True, with_mate), (False, alone)):
            members = [zz for zz in range(zs) if test(zz, o) and zz != but and only in (None, zz)]
            if members:
                pl.when(one_of(members))(functools.partial(mix, members, paired))

        if only is not None:
            return

        @pl.when(one_of([zz for zz in (0, zs - 1) if zz != o]))
        def _():
            @pl.loop(low, high)
            def _(g):
                arrived(mixed_v.at[g, :, o], ret_r.at[g, o])
                for b in range(blocks):
                    spot = slice(b * block + lo, b * block + lo + zr)
                    gated_v[g, spot, :] = (
                        open_v[g, spot, :] * mixed_v[g, b, o].astype(jnp.float32)
                    ).astype(jnp.bfloat16)
                hand_over(g, o)

    def plane_round(zz):
        for o in others(zz):
            for r in range(1, sp):
                if not (square and r == 3):
                    arrived(ow_piece(source(r), o, c), pl_r.at[r, o])
            go(plane_second(zz, o))
            for r in range(1, sp):
                if not (square and r == 3):
                    go(plane_pair(r, o))

    def plane_end(zz):
        for o in others(zz):
            for p in range(parts):
                arrived(second_part(source(3), o, p), p2_r.at[o, p])
            go(plane_pair(3, o))

    each_z(plane_round)

    unit(zs - 1, only=zs - 1)
    for o in range(zs - 1):
        unit(o)
        if o == 0 and held_back < groups:
            each_d(late_mix, lambda zz: late(zz, zz + 1))

    if square:
        each_z(plane_end)

    def gather_part(p):
        for s in range(sp):
            @pl.when(me != s)
            def _():
                arrived(held_v.at[s, pl.ds(p * per_part, per_part)], ga_r.at[p, s])
        squares = jnp.zeros((per, gd), jnp.float32)
        for s in range(sp):
            for i in range(per_part):
                g = p * per_part + i
                value = held_v[s, g].astype(jnp.float32)
                squares += value * value
                cols = slice(s * chans + g * gd, s * chans + (g + 1) * gd)
                normed_v[p, :, s * pk + i * gd:s * pk + (i + 1) * gd] = (
                    value * ogain_ref[:, cols]).astype(jnp.bfloat16)
        sums_v[...] = squares if p == 0 else sums_v[...] + squares

    def part_dot(p, cols):
        return jnp.dot(normed_v[p], outw_v[p, :, :, cols].reshape(sp * pk, ncol),
                       preferred_element_type=jnp.float32)

    def weights_here():
        arrived(outw_v.at[:, :, :, own_cols], ow_own.at[1])
        arrived(ow_bytes(zs - 1), ow_pr.at[0])
        for r in range(1, sp):
            arrived(ow_bytes(zs - 1), pp_r.at[r])

    weights_here()
    if parts > 1:
        unit(zs - 1, 0, groups - 1, but=zs - 1)
        gather_part(0)

        @pl.loop(0, width // ncol)
        def _(t):
            cols = pl.ds(pl.multiple_of(t * ncol, LANES), ncol)
            part_v[:, cols] = part_dot(0, cols)

        unit(zs - 1, groups - 1, groups, but=zs - 1)
    else:
        unit(zs - 1, but=zs - 1)
    gather_part(parts - 1)
    scale = lax.rsqrt(jnp.sum(sums_v[...], axis=-1, keepdims=True) / (sp * chans) + norm_eps)

    @pl.loop(0, width // ncol)
    def _(t):
        cols = pl.ds(pl.multiple_of(t * ncol, LANES), ncol)
        last = part_dot(parts - 1, cols)
        if parts > 1:
            last += part_v[:, cols]
        out_ref[:, cols] = (last * scale).astype(jnp.bfloat16)

    sent(tok_v.at[pl.ds(0, sp - 1)], tok_s.at[0])
    sent(outw_v.at[:, :, :, own_cols], ow_own.at[0])
    for r in range(1, sp):
        if not (square and r == 3):
            sent(ow_bytes(zs - 1), pl_s.at[r])
        sent(ow_bytes(zs - 1), pp_s.at[r])
    if square:
        sent(ow_bytes(zs - 1), p2_s.at[0])
    sent(ow_bytes(zs - 1), ow_send.at[2])
    sent(ug_v.at[pl.ds(0, zs * depth), :], ug_send.at[2])
    sent(held_v.at[pl.ds(0, sp - 1)], ga_s.at[0])

    def line_sent(zz):
        for n, way in ((zz + 1 if zz < zs - 1 else 0, 0), (zs - zz if zz > 0 else 0, 1)):
            if n:
                sent(ug_v.at[pl.ds(0, n * depth), :], ug_send.at[way])
                sent(ow_bytes(n), ow_send.at[way])
        if not inner(zz):
            n = sum(v_useful(zz, q) for q in range(sp))
            sent(norm_v.at[:, pl.ds(0, n * per), :], v_s.at[0])
        elif mate(zz) is not None:
            n = sum(with_mate(zz, o) for o in range(zs))
            sent(mixed_v.at[:, :, pl.ds(0, n)], ret_s.at[0])

    each_z(line_sent)

    def mix_sent(zz, cc):
        for o in range(zs):
            d = o * CORES + cc
            for i, (r0, rn, cols) in enumerate(cuts(d)):
                spot = mix_v.at[:, d, pl.ds(r0, rn), pl.ds(0, cols)]
                if not (inner(zz) or o == zz):
                    continue
                if o >= zz and inner(zz - 1):
                    sent(spot, mx_dn.at[o, i])
                if o <= zz and inner(zz + 1):
                    sent(spot, mx_up.at[o, i])
                sent(spot, mx_ps.at[o, i])

    each_d(mix_sent)


def body(tokens, up_weight, gate_weight, group_gain, mix_weight, mix_bias, out_gain, out_weight):
    per, width = tokens.shape[1:]
    groups, gd = group_gain.shape
    rows, block = mix_weight.shape[1:]
    sp, dps = lax.axis_size("sp"), lax.axis_size("dp")
    zs = dps // CORES
    total = sp * per
    parts = 1 if groups % 2 else 2
    bf, f32 = jnp.bfloat16, jnp.float32
    dma = pltpu.SemaphoreType.DMA
    hbm = pl.BlockSpec(memory_space=pltpu.HBM)
    vmem = pl.BlockSpec(memory_space=pltpu.VMEM)
    output = pl.pallas_call(
        functools.partial(fused_kernel, sp, zs),
        out_shape=pltpu.VMEM((per, width), bf),
        in_specs=[hbm, hbm, hbm, vmem, hbm, vmem, vmem, hbm],
        out_specs=vmem,
        scratch_shapes=[
            pltpu.VMEM((sp, per, width), bf),
            pltpu.VMEM((width, 2 * groups * gd), bf),
            pltpu.VMEM((groups, dps, rows, block), bf),
            pltpu.VMEM((parts, sp, groups * gd // parts, width), bf),
            pltpu.VMEM((groups, total, gd), f32),
            pltpu.VMEM((groups, total, gd), bf),
            pltpu.VMEM((groups, total, gd), bf),
            pltpu.VMEM((groups, block, gd), f32),
            pltpu.VMEM((groups, total // block, zs, CORES * rows, gd), bf),
            pltpu.VMEM((groups, total, gd), bf),
            pltpu.VMEM((sp, groups, per, gd), bf),
            pltpu.VMEM((parts, per, sp * groups * gd // parts), bf),
            pltpu.VMEM((per, gd), f32),
            pltpu.VMEM((per, width if parts > 1 else gd), f32),
            dma((4,)),
            dma((zs, 2)), dma((3,)), dma((1,)),
            dma((zs,)), dma((3,)), dma((1,)), dma((2,)),
            dma((sp,)), dma((sp, zs)), dma((1,)), dma((zs, parts)), dma((sp,)), dma((sp,)),
            dma((groups, zs, 2)), dma((groups, zs, 2)), dma((zs, 2)), dma((zs, 2)), dma((zs, 2)),
            dma((1,)), dma((sp, 2)), dma((1,)), dma((sp,)),
            dma((1,)), dma((groups, zs)), dma((1,)), dma((parts, sp)),
        ],
        compiler_params=pltpu.CompilerParams(collective_id=0, has_side_effects=True, vmem_limit_bytes=65_000_000),
    )(tokens.reshape(per, width), up_weight, gate_weight, group_gain[:, None, :], mix_weight, mix_bias,
      out_gain[None, :], out_weight.reshape(sp, parts, groups * gd // parts, -1))
    return output.reshape(tokens.shape)


def solution(mesh):
    return jax.shard_map(
        body,
        mesh=mesh,
        in_specs=(
            P("dp", "sp", None),
            P("dp", None),
            P("dp", None),
            P("sp", None),
            P("sp", "dp", None),
            P("sp", None),
            P(),
            P(None, "dp"),
        ),
        out_specs=P("dp", "sp", None),
        check_vma=False,
    )
```

```python
import functools

import jax
import jax.numpy as jnp
from jax import lax
from jax.experimental import pallas as pl
from jax.experimental.pallas import tpu as pltpu
from jax.sharding import PartitionSpec as P

norm_eps = 1e-06
CORES = 2
LANES = 128
MESH = pl.DeviceIdType.MESH


def up_to(n, m):
    return -(-n // m) * m


def fused_kernel(
    sp, zs,
    tok_ref, up_ref, gate_ref, gain_ref, mix_ref, bias_ref, ogain_ref, outw_ref, out_ref,
    tok_v, ug_v, mix_v, outw_v, open_v, norm_v, other_v, bias_v, mixed_v, gated_v, held_v,
    normed_v, sums_v, part_v, far_v, far_m,
    load_sem, ug_line, ug_send, ug_pr, ow_line, ow_send, ow_pr, ow_own,
    pl_s, pl_r, p2_s, p2_r, pp_s, pp_r, mx_line, mx_pr, mx_up, mx_dn, mx_ps,
    tok_s, tok_r, v_s, v_r, ret_s, ret_r, ga_s, ga_r, fv_s, fv_r, fm_s, fm_r,
):
    me = lax.axis_index("sp")
    dp = lax.axis_index("dp")
    z, c = dp // CORES, lax.rem(dp, CORES)
    groups, dps, rows, block = mix_v.shape
    per, width = out_ref.shape
    gd = gain_ref.shape[2]
    chans = groups * gd
    depth, ncol = up_ref.shape[0], outw_ref.shape[3]
    total = sp * per
    blocks = total // block
    parts, _, pk, _ = outw_v.shape
    halves = 1 if parts % 2 else 2
    hp = parts // halves
    zr = CORES * rows
    half, dhalf = per // 2, depth // 2
    square = sp == 4
    far = zs == 4 and groups > 2
    below, above, last_g = zs // 2 - 1, zs // 2, groups - 1

    partner = {"dp": z * CORES + (1 - c)}

    def at_line(zz):
        return {"dp": zz * CORES + c}

    def around(r, sign):
        if square:
            y = lax.rem(me // 2 + r // 2, 2)
            x = lax.rem(lax.rem(me, 2) + r % 2, 2)
            return y * 2 + x
        return lax.rem(me + sign * r + sp, sp)

    def target(r):
        return around(r, 1)

    def source(r):
        return around(r, -1)

    def peer(r):
        return {"sp": target(r)}

    def inner(zz):
        return 0 < zz < zs - 1

    def mate(zz):
        return {0: 1, 1: 0, zs - 1: zs - 2, zs - 2: zs - 1}.get(zz)

    def remote(src, dst, send, recv, device):
        return pltpu.make_async_remote_copy(
            src_ref=src, dst_ref=dst, send_sem=send, recv_sem=recv,
            device_id=device, device_id_type=MESH)

    def sent(ref, sem):
        remote(ref, ref, sem, sem, partner).wait_send()

    def arrived(ref, sem):
        remote(ref, ref, sem, sem, partner).wait_recv()

    def each_z(fn, only=None):
        for zz in range(zs):
            if only is None or only(zz):
                pl.when(z == zz)(functools.partial(fn, zz))

    def each_d(fn, only=None):
        for zz in range(zs):
            if only is None or only(zz):
                for cc in range(CORES):
                    pl.when(dp == zz * CORES + cc)(functools.partial(fn, zz, cc))

    loads = {"ug": [], "tok": [], "ow": [], "mx": []}
    for g in range(groups):
        for t, ref in enumerate((up_ref, gate_ref)):
            cols = pl.ds(pl.multiple_of(me * chans + g * gd, LANES), gd)
            spot = 2 * g + t
            loads["ug"].append(pltpu.make_async_copy(
                ref.at[:, cols],
                ug_v.at[pl.ds(dp * depth, depth), pl.ds(spot * gd, gd)],
                load_sem.at[3]))
    loads["tok"].append(pltpu.make_async_copy(tok_ref, tok_v.at[me], load_sem.at[0]))
    own_cols = pl.ds(pl.multiple_of(dp * ncol, LANES), ncol)
    for p in range(parts):
        loads["ow"].append(pltpu.make_async_copy(
            outw_ref.at[:, p], outw_v.at[p, :, :, own_cols], load_sem.at[1]))
    loads["mx"].append(pltpu.make_async_copy(mix_ref, mix_v.at[:, dp], load_sem.at[2]))
    for kind in ("ug", "tok", "ow", "mx"):
        for load in loads[kind]:
            load.start()

    def loaded(ref, sem):
        pltpu.make_async_copy(ref, ref, sem).wait()

    barrier = pltpu.get_barrier_semaphore()

    def greet(zz):
        friends = [partner] + [peer(r) for r in range(1, sp)]
        if zz > 0:
            friends.append(at_line(zz - 1))
        if zz < zs - 1:
            friends.append(at_line(zz + 1))
        for friend in friends:
            pl.semaphore_signal(barrier, inc=1, device_id=friend, device_id_type=MESH)
        pl.semaphore_wait(barrier, len(friends))

    each_z(greet)

    def ug_piece(o, cc, h):
        return ug_v.at[pl.ds((o * CORES + cc) * depth + h * dhalf, dhalf), :]

    def ow_piece(s, o, cc):
        cols = pl.ds(pl.multiple_of((o * CORES + cc) * ncol, LANES), ncol)
        return outw_v.at[:, s, :, cols]

    def cuts(d):
        out, at, end = [], d * rows, (d + 1) * rows
        while at < end:
            top = min(end, (at // LANES + 1) * LANES)
            out.append((at - d * rows, top - at, min(block, up_to(top, LANES))))
            at = top
        return out

    def mx_bytes(d):
        size = sum(rn * cols for _, rn, cols in cuts(d))
        return open_v.at[0, pl.ds(0, size // gd // 2), :]

    def mx_piece(g, d, piece):
        r0, rn, cols = piece
        return mix_v.at[g, d, pl.ds(r0, rn), pl.ds(0, cols)]

    def ug_copies(zz, o, h):
        src, out = ug_piece(o, c, h), []
        if o >= zz and zz > 0:
            out.append(remote(src, src, ug_send.at[1], ug_line.at[o, h], at_line(zz - 1)))
        if o <= zz and zz < zs - 1:
            out.append(remote(src, src, ug_send.at[0], ug_line.at[o, h], at_line(zz + 1)))
        out.append(remote(src, src, ug_send.at[2], ug_pr.at[0], partner))
        return out

    def ow_down(zz, o):
        src = ow_piece(me, o, c)
        if o >= zz and zz > 0:
            return [remote(src, src, ow_send.at[1], ow_line.at[o], at_line(zz - 1))]
        return []

    def ow_rise(zz, o):
        src = ow_piece(me, o, c)
        if o <= zz and zz < zs - 1:
            return [remote(src, src, ow_send.at[0], ow_line.at[o], at_line(zz + 1))]
        return []

    def ow_pair(o):
        src = ow_piece(me, o, c)
        return [remote(src, src, ow_send.at[2], ow_pr.at[0], partner)]

    def ow_own_pair():
        src = outw_v.at[:, :, :, own_cols]
        return [remote(src, src, ow_own.at[0], ow_own.at[1], partner)]

    def ow_bytes(n):
        return outw_v.at[:, 0, :, pl.ds(0, n * ncol)]

    def mx_copies(zz, cc, g, o, way):
        out = []
        d = o * CORES + cc
        for i, piece in enumerate(cuts(d)):
            src = mx_piece(g, d, piece)
            if way == "dn" and o >= zz and inner(zz - 1):
                out.append(remote(src, src, mx_dn.at[o, i], mx_line.at[g, o], at_line(zz - 1)))
            if way == "up" and o <= zz and inner(zz + 1):
                out.append(remote(src, src, mx_up.at[o, i], mx_line.at[g, o], at_line(zz + 1)))
            if way == "pair" and (inner(zz) or o == zz):
                out.append(remote(src, src, mx_ps.at[o, i], mx_pr.at[g, o], partner))
        return out

    def go(copies):
        for copy in copies:
            copy.start()

    def own_mix(zz, way, low=0, high=groups):
        if far and zz == above and way == "dn":
            high = min(high, last_g)

        for cc in range(CORES):
            @pl.when(c == cc)
            def _():
                @pl.loop(low, high)
                def _(g):
                    go(mx_copies(zz, cc, g, zz, way))

    def ug_left(zz, way, k):
        far = zs - 1 - zz if way == "dn" else zz
        there = zz > 0 if way == "dn" else zz < zs - 1
        return there, max(0, far - k)

    held_back = max(1, groups - 1)

    def own_out(zz, way):
        go(ow_down(zz, zz) if way == "dn" else ow_rise(zz, zz))

    loaded(ug_v.at[pl.ds(dp * depth, depth), :], load_sem.at[3])

    def first_weights(zz):
        for h in range(2):
            go(ug_copies(zz, zz, h))

    each_z(first_weights)
    for load in loads["tok"]:
        load.wait()

    def tok_half(s, h):
        return tok_v.at[s, pl.ds(h * half, half), :]

    def tok_copy(s, r, h, r_there):
        return remote(tok_half(s, h), tok_half(s, h), tok_s.at[0], tok_r.at[r_there, h], peer(r))

    def tok_first():
        if square:
            return [tok_copy(me, 1, 0, 1), tok_copy(me, 2, 1, 2), tok_copy(me, 1, 1, 1), tok_copy(me, 2, 0, 2)]
        return [tok_copy(me, r, h, r) for r in range(1, sp) for h in range(2)]

    def tok_second():
        if square:
            return [tok_copy(source(1), 2, 0, 3), tok_copy(source(2), 1, 1, 3)]
        return []

    go(tok_first())
    loaded(outw_v.at[:, :, :, own_cols], load_sem.at[1])
    loads["mx"][0].wait()
    go(ow_own_pair())

    def first_rest(zz):
        for way in ("dn", "up"):
            there, left = ug_left(zz, way, 0)
            if there and left == 0:
                own_out(zz, way)
                own_mix(zz, way, 0, held_back if zz == zs - 1 else groups)
        own_mix(zz, "pair")

    each_z(first_rest)

    for g in range(groups):
        for t in range(block // LANES):
            spot = slice(t * LANES, (t + 1) * LANES)
            bias_v[g, spot, :] = jnp.broadcast_to(bias_ref[g:g + 1, spot], (gd, LANES)).T

    def take_ug(zz, k):
        for o in (zz + k, zz - k):
            if 0 <= o < zs:
                for h in range(2):
                    arrived(ug_piece(o, c, h), ug_line.at[o, h])
                    go(ug_copies(zz, o, h))
        for way in ("dn", "up"):
            there, left = ug_left(zz, way, k)
            before = ug_left(zz, way, k - 1)[1]
            if there and left == 0 and before > 0:
                own_out(zz, way)
                own_mix(zz, way, 0, 1)

    def take_out(zz, k):
        for o in (zz + k, zz - k):
            if 0 <= o < zs:
                arrived(ow_piece(me, o, c), ow_line.at[o])
                go(ow_down(zz, o) if o > zz else ow_rise(zz, o))
                go(ow_pair(o))
        for way in ("dn", "up"):
            there, left = ug_left(zz, way, k)
            before = ug_left(zz, way, k - 1)[1]
            if there and left == 0 and before > 0:
                own_mix(zz, way, 1, groups)

    def others(zz):
        return [o for k in range(1, zs) for o in (zz + k, zz - k) if 0 <= o < zs]

    def plane_first(o):
        src = ow_piece(me, o, c)
        reach = (1, 2) if square else range(1, sp)
        return [remote(src, src, pl_s.at[r], pl_r.at[r, o], peer(r)) for r in reach]

    def second_part(s, o, p):
        cols = pl.ds(pl.multiple_of((o * CORES + c) * ncol, LANES), ncol)
        return outw_v.at[pl.ds(p * hp, hp), s, :, cols]

    def plane_second(zz, o):
        if not square:
            return []
        units = [(x, p) for x in others(zz) for p in range(halves)]
        out = []
        for p in range(halves):
            via, to = (1, 2) if units.index((o, p)) < len(units) // 2 else (2, 1)
            src = second_part(source(via), o, p)
            out.append(remote(src, src, p2_s.at[0], p2_r.at[o, p], peer(to)))
        return out

    def plane_pair(r, o):
        src = ow_piece(source(r), o, c)
        return [remote(src, src, pp_s.at[r], pp_r.at[r], partner)]

    each_z(lambda zz: take_ug(zz, 1))
    if square:
        arrived(tok_half(source(1), 0), tok_r.at[1, 0])
        arrived(tok_half(source(2), 1), tok_r.at[2, 1])
    go(tok_second())

    def more_weights(zz):
        for k in range(2, zs):
            take_ug(zz, k)
        if inner(zz) and not square:
            for k in range(1, zs):
                take_out(zz, k)
            for o in others(zz):
                go(plane_first(o))

    each_z(more_weights)

    arrived(ug_v.at[pl.ds(0, zs * depth), :], ug_pr.at[0])

    def split(zz):
        return far and zz == below - 1

    def v_copies(zz, q):
        spot = pl.ds(pl.multiple_of(q * per, 16), per)
        ranges = ((last_g, 1), (0, last_g)) if split(zz) else ((0, groups),)
        out = []
        for i, (g0, gn) in enumerate(ranges):
            which = len(ranges) - 1 - i
            src, dst = (ref.at[pl.ds(g0, gn), spot, :] for ref in (norm_v, other_v))
            out.append(remote(src, dst, v_s.at[which], v_r.at[which, q], at_line(mate(zz))))
        return out

    def starts(q):
        return (q * per) % block

    def v_useful(end, q):
        return any(starts(q) < (o + 1) * zr for o in range(zs) if o != end) or block % per > 0

    def send_v(zz, s):
        for q in range(sp):
            if v_useful(zz, q):
                pl.when(s == q)(lambda q=q: go(v_copies(zz, q)))

    def far_send(i, ref):
        return remote(ref.at[last_g], far_v.at[i], fv_s.at[i], fv_r.at[i], at_line(above))

    def project(s):
        spot = pl.ds(pl.multiple_of(s * per, 16), per)

        @pl.loop(0, groups)
        def _(g):
            cols = pl.ds(pl.multiple_of(g * 2 * gd, 2 * gd), 2 * gd)
            both = jnp.dot(tok_v[s], ug_v[:, cols], preferred_element_type=jnp.float32)
            both = jax.nn.gelu(both.astype(jnp.bfloat16).astype(jnp.float32))
            open_v[g, spot, :] = both[:, :gd]
            act = both[:, gd:]
            act = act - jnp.mean(act, axis=-1, keepdims=True)
            spread = jnp.mean(act * act, axis=-1, keepdims=True)
            norm_v[g, spot, :] = (
                act * lax.rsqrt(spread + norm_eps) * gain_ref[g]
            ).astype(jnp.bfloat16)

        each_z(lambda zz: send_v(zz, s), lambda zz: not inner(zz))

    def out_events(zz, ks):
        for k in ks:
            take_out(zz, k)
            for o in (zz + k, zz - k):
                if 0 <= o < zs:
                    go(plane_first(o))

    if square:
        def in_order(i):
            place = jnp.where(me == sp - 1, 1 - i, i) if i < 2 else i
            return jnp.where((z == 0) | (z == zs - 1), source(place), i)

        for r in range(sp):
            turn = in_order(r)
            for h in range(2):
                @pl.when((turn > 0) & (turn != 1 + h))
                def _():
                    arrived(tok_half(source(turn), h), tok_r.at[turn, h])
            project(source(turn))

            def events(zz, r=r):
                first = r + 1 if inner(zz) else r
                ks = range(first, zs if r == sp - 1 else first + 1)
                out_events(zz, [k for k in ks if 0 < k < zs])

            each_z(events)
    else:
        @pl.loop(0, sp)
        def _(r):
            @pl.when(r > 0)
            def _():
                for h in range(2):
                    arrived(tok_half(source(r), h), tok_r.at[r, h])

            project(source(r))

        each_z(lambda zz: out_events(zz, range(1, zs)), lambda zz: not inner(zz))

    def take_mix(zz, cc, g, o, onward=True):
        d = o * CORES + cc
        arrived(mx_bytes(d), mx_line.at[g, o])
        if onward:
            go(mx_copies(zz, cc, g, o, "dn" if o > zz else "up"))
        go(mx_copies(zz, cc, g, o, "pair"))

    def passed_on(zz, o):
        return abs(o - zz) == 1 and inner(zz - 1 if o > zz else zz + 1)

    def late(zz, o):
        return zz == zs - 2 and o == zs - 1

    def near_mix(zz, cc):
        for o in (zz + 1, zz - 1):
            if passed_on(zz, o):
                @pl.loop(0, held_back if late(zz, o) else groups)
                def _(g):
                    take_mix(zz, cc, g, o)

    def late_mix(zz, cc):
        @pl.loop(held_back, groups)
        def _(g):
            take_mix(zz, cc, g, zz + 1, not far)

    each_d(near_mix, inner)
    if far:
        each_z(lambda zz: far_send(0, norm_v).start(), lambda zz: zz == below)

    def ready_at(q):
        if block % per:
            return zs - 1
        return (((q + 1) * per - 1) % block) // zr

    def needs(o):
        return min(block, up_to((o + 1) * zr, LANES))

    def first_need(zz, q):
        if not v_useful(mate(zz), q):
            return None
        return next(o for o in range(zs) if o != mate(zz) and (block % per or starts(q) < (o + 1) * zr))

    def with_mate(zz, o):
        return inner(zz) and mate(zz) is not None and mate(zz) != o

    def alone(zz, o):
        return zz == o if not inner(zz) else not with_mate(zz, o)

    def gated_copy(g, q):
        return remote(gated_v.at[g, pl.ds(q * per, per), :], held_v.at[me, g],
                      ga_s.at[0], ga_r.at[g, me], {"sp": q})

    def ret_copy(zz, g, o):
        spot = mixed_v.at[g, :, o]
        return remote(spot, spot, ret_s.at[0], ret_r.at[g, o], at_line(mate(zz)))

    def hand_over(g, o):
        for q in range(sp):
            if ready_at(q) == o:
                @pl.when(me == q)
                def _():
                    held_v[q, g] = gated_v[g, pl.ds(q * per, per), :]

                @pl.when(me != q)
                def _():
                    gated_copy(g, q).start()

    def one_of(zs_in):
        return functools.reduce(jnp.logical_or, [z == zz for zz in zs_in])

    def unit(o, low=0, high=groups, only=None, but=()):
        lo = o * zr
        base, top = lo // LANES * LANES, needs(o)

        def wait_v(zz):
            apart = split(mate(zz))
            for q in range(sp):
                if first_need(zz, q) == o:
                    rows_of = pl.ds(q * per, per)
                    main = pl.ds(0, last_g if apart else groups)
                    arrived(other_v.at[main, rows_of, :], v_r.at[0, q])
                    if apart and o < above:
                        arrived(other_v.at[pl.ds(last_g, 1), rows_of, :], v_r.at[1, q])

        if low == 0:
            each_z(wait_v, lambda zz: with_mate(zz, o) and zz not in but and only in (None, zz))

        def mix(members, paired):
            def rows_from_line(zz, cc):
                @pl.loop(low, high)
                def _(g):
                    take_mix(zz, cc, g, o)

            each_d(rows_from_line, lambda zz: zz in members and o != zz and not passed_on(zz, o))

            @pl.loop(low, high)
            def _(g):
                def rows_in(zz, cc):
                    if not (far and zz == above and o == zs - 1 and low == last_g):
                        arrived(mx_bytes(o * CORES + 1 - cc), mx_pr.at[g, o])

                def values(at, end, spare=0):
                    own = norm_v[g, at:end, :]
                    if not paired:
                        return own
                    other = other_v[g, at:end - spare, :]
                    if spare:
                        zeros = jnp.zeros((spare, gd), jnp.bfloat16)
                        other = jnp.concatenate([other, zeros], axis=0)
                    return jnp.concatenate([own, other], axis=1)

                each_d(rows_in, lambda zz: zz in members)
                corner = mix_v[g, o * CORES:(o + 1) * CORES, :, base:top].reshape(zr, top - base)
                keep = lax.broadcasted_iota(jnp.int32, corner.shape, 0) + (lo - base) >= (
                    lax.broadcasted_iota(jnp.int32, corner.shape, 1))
                corner = jnp.where(keep, corner.astype(jnp.float32), 0.0).astype(jnp.bfloat16)
                bias = bias_v[g, lo:lo + zr, :]
                for b in range(blocks):
                    at = b * block
                    mixed = jnp.dot(corner, values(at + base, at + top, top - lo - zr),
                                    preferred_element_type=jnp.float32)
                    if base > 0:
                        left = mix_v[g, o * CORES:(o + 1) * CORES, :, :base].reshape(zr, base)
                        mixed += jnp.dot(left, values(at, at + base),
                                         preferred_element_type=jnp.float32)
                    spot = slice(at + lo, at + lo + zr)
                    if paired:
                        mixed_v[g, b, o] = (mixed[:, gd:] + bias).astype(jnp.bfloat16)
                    gated_v[g, spot, :] = (
                        open_v[g, spot, :] * (mixed[:, :gd] + bias)).astype(jnp.bfloat16)
                if paired:
                    each_z(lambda zz: ret_copy(zz, g, o).start(), lambda zz: zz in members)
                hand_over(g, o)

        for paired, test in ((True, with_mate), (False, alone)):
            members = [zz for zz in range(zs) if test(zz, o) and zz not in but and only in (None, zz)]
            if members:
                pl.when(one_of(members))(functools.partial(mix, members, paired))

        if only is not None:
            return

        waiting = [zz for zz in (0, zs - 1) if zz != o and zz not in but]
        if not waiting:
            return

        @pl.when(one_of(waiting))
        def _():
            @pl.loop(low, high)
            def _(g):
                arrived(mixed_v.at[g, :, o], ret_r.at[g, o])
                for b in range(blocks):
                    spot = slice(b * block + lo, b * block + lo + zr)
                    gated_v[g, spot, :] = (
                        open_v[g, spot, :] * mixed_v[g, b, o].astype(jnp.float32)
                    ).astype(jnp.bfloat16)
                hand_over(g, o)

    def plane_round(zz):
        for n, o in enumerate(others(zz)):
            if n == 1 and zz == zs - 1 and held_back < groups:
                own_mix(zz, "dn", held_back, groups)
            for r in range(1, sp):
                if not (square and r == 3):
                    arrived(ow_piece(source(r), o, c), pl_r.at[r, o])
            go(plane_second(zz, o))
            for r in range(1, sp):
                if not (square and r == 3):
                    go(plane_pair(r, o))

    def plane_end(zz):
        for o in others(zz):
            for p in range(halves):
                arrived(second_part(source(3), o, p), p2_r.at[o, p])
            go(plane_pair(3, o))

    def far_forward(zz):
        for q in range(sp):
            if first_need(zz, q) >= above:
                arrived(other_v.at[pl.ds(last_g, 1), pl.ds(q * per, per), :], v_r.at[1, q])
        far_send(1, other_v).start()

    def far_unit(i):
        o = above + i
        lo, top = o * zr, needs(o)
        base = lo // LANES * LANES
        rows_of = slice(o * CORES, (o + 1) * CORES)
        corner = mix_v[last_g, rows_of, :, base:top].reshape(zr, top - base)
        keep = lax.broadcasted_iota(jnp.int32, corner.shape, 0) + (lo - base) >= (
            lax.broadcasted_iota(jnp.int32, corner.shape, 1))
        corner = jnp.where(keep, corner.astype(jnp.float32), 0.0).astype(jnp.bfloat16)
        left = mix_v[last_g, rows_of, :, :base].reshape(zr, base)
        bias = bias_v[last_g, lo:lo + zr, :]

        def values(at, end):
            return jnp.concatenate([far_v[0, at:end, :], far_v[1, at:end, :]], axis=1)

        for b in range(blocks):
            at = b * block
            mixed = jnp.dot(left, values(at, at + base), preferred_element_type=jnp.float32)
            mixed += jnp.dot(corner, values(at + base, at + top), preferred_element_type=jnp.float32)
            for n in range(2):
                far_m[n, i, b] = (mixed[:, n * gd:(n + 1) * gd] + bias).astype(jnp.bfloat16)

    def far_back(i):
        spot = far_m.at[:, i]
        return remote(spot, spot, fm_s.at[i], fm_r.at[i], at_line(below))

    def far_above(zz):
        for i in range(2):
            arrived(far_v.at[i], fv_r.at[i])
        for cc in range(CORES):
            @pl.when(c == cc)
            def _():
                arrived(mx_bytes((zs - 1) * CORES + 1 - cc), mx_pr.at[last_g, zs - 1])
        for i in range(2):
            far_unit(i)
            far_back(i).start()

    def far_ret(i):
        return remote(far_m.at[1, i], mixed_v.at[last_g, :, above + i],
                      ret_s.at[0], ret_r.at[last_g, above + i], at_line(below - 1))

    def far_below(zz):
        for i in range(2):
            o = above + i
            if zz == below:
                arrived(far_m.at[:, i], fm_r.at[i])
                far_ret(i).start()
            else:
                arrived(mixed_v.at[last_g, :, o], ret_r.at[last_g, o])
            for b in range(blocks):
                spot = slice(b * block + o * zr, b * block + (o + 1) * zr)
                mixed = far_m[0, i, b] if zz == below else mixed_v[last_g, b, o]
                gated_v[last_g, spot, :] = (
                    open_v[last_g, spot, :] * mixed.astype(jnp.float32)).astype(jnp.bfloat16)
            hand_over(last_g, o)

    ends, insides = (0, zs - 1), tuple(range(1, zs - 1))
    unit(zs - 1, 0, held_back, only=zs - 2)
    for o in range(zs // 2):
        unit(o, but=ends)
    if far:
        each_z(far_forward, lambda zz: zz == below)
    each_z(plane_round)

    unit(zs - 1, only=zs - 1)
    lower = (below - 1, below)
    for o in range(zs - 1):
        if o < zs // 2:
            unit(o, but=insides)
        elif far and o == above:
            unit(o, 0, last_g)
            unit(o, last_g, groups, but=lower)
        else:
            unit(o)
    if held_back < groups:
        each_d(late_mix, lambda zz: late(zz, zz + 1))
    if far:
        each_z(far_above, lambda zz: zz == above)

    def gather_part(g, first):
        for s in range(sp):
            @pl.when(me != s)
            def _():
                arrived(held_v.at[s, g], ga_r.at[g, s])
        squares = jnp.zeros((per, gd), jnp.float32)
        for s in range(sp):
            value = held_v[s, g].astype(jnp.float32)
            squares += value * value
            cols = slice(s * chans + g * gd, s * chans + (g + 1) * gd)
            normed_v[g, :, s * pk:(s + 1) * pk] = (value * ogain_ref[:, cols]).astype(jnp.bfloat16)
        sums_v[...] = squares if first else sums_v[...] + squares

    def part_dot(p, cols):
        return jnp.dot(normed_v[p], outw_v[p, :, :, cols].reshape(sp * pk, ncol),
                       preferred_element_type=jnp.float32)

    def weights_here():
        arrived(outw_v.at[:, :, :, own_cols], ow_own.at[1])
        arrived(ow_bytes(zs - 1), ow_pr.at[0])
        for r in range(1, sp):
            arrived(ow_bytes(zs - 1), pp_r.at[r])

    def plane_done():
        if square:
            each_z(plane_end)
        weights_here()

    started = []

    def add_parts(which):
        for g in which:
            gather_part(g, not started)
            started.append(g)

        @pl.loop(0, width // ncol)
        def _(t):
            cols = pl.ds(pl.multiple_of(t * ncol, LANES), ncol)
            more = sum(part_dot(p, cols) for p in which)
            part_v[:, cols] = more if len(started) == len(which) else part_v[:, cols] + more

    done = (zs - 1, zs - 2)
    if far:
        unit(zs - 1, 0, last_g - 1, but=done)
        early = (me < sp - 1) & ((z == 0) | (z == zs - 1))

        def first_parts():
            started.clear()
            plane_done()
            add_parts(range(last_g - 1))

        pl.when(early)(first_parts)
        each_z(far_below, lambda zz: zz in lower)
        unit(zs - 1, last_g - 1, last_g, but=done)
        unit(zs - 1, last_g, groups, but=lower + (zs - 1,))
        pl.when(jnp.logical_not(early))(first_parts)
        add_parts([last_g])
        final = last_g - 1
    elif groups > 1:
        plane_done()
        unit(zs - 1, 0, last_g, but=done)
        add_parts(range(last_g))
        unit(zs - 1, last_g, groups, but=(zs - 1,))
        final = last_g
    else:
        plane_done()
        unit(zs - 1, but=done)
        final = 0
    gather_part(final, not started)
    scale = lax.rsqrt(jnp.sum(sums_v[...], axis=-1, keepdims=True) / (sp * chans) + norm_eps)

    @pl.loop(0, width // ncol)
    def _(t):
        cols = pl.ds(pl.multiple_of(t * ncol, LANES), ncol)
        last = part_dot(final, cols)
        if started:
            last += part_v[:, cols]
        out_ref[:, cols] = (last * scale).astype(jnp.bfloat16)

    sent(tok_v.at[pl.ds(0, sp - 1)], tok_s.at[0])
    sent(outw_v.at[:, :, :, own_cols], ow_own.at[0])
    for r in range(1, sp):
        if not (square and r == 3):
            sent(ow_bytes(zs - 1), pl_s.at[r])
        sent(ow_bytes(zs - 1), pp_s.at[r])
    if square:
        sent(ow_bytes(zs - 1), p2_s.at[0])
    sent(ow_bytes(zs - 1), ow_send.at[2])
    sent(ug_v.at[pl.ds(0, zs * depth), :], ug_send.at[2])
    sent(held_v.at[pl.ds(0, sp - 1)], ga_s.at[0])

    def line_sent(zz):
        for n, way in ((zz + 1 if zz < zs - 1 else 0, 0), (zs - zz if zz > 0 else 0, 1)):
            if n:
                sent(ug_v.at[pl.ds(0, n * depth), :], ug_send.at[way])
                sent(ow_bytes(n), ow_send.at[way])
        if not inner(zz):
            n = sum(v_useful(zz, q) for q in range(sp))
            main = pl.ds(0, last_g if split(zz) else groups)
            sent(norm_v.at[main, pl.ds(0, n * per), :], v_s.at[0])
            if split(zz):
                sent(norm_v.at[pl.ds(0, 1), pl.ds(0, n * per), :], v_s.at[1])
        elif mate(zz) is not None:
            n = sum(with_mate(zz, o) for o in range(zs))
            sent(mixed_v.at[:, :, pl.ds(0, n)], ret_s.at[0])
        for i in range(2):
            if far and zz == below:
                sent(far_v.at[i], fv_s.at[i])
            if far and zz == above:
                sent(far_m.at[:, i], fm_s.at[i])

    each_z(line_sent)

    def mix_sent(zz, cc):
        for o in range(zs):
            d = o * CORES + cc
            for i, (r0, rn, cols) in enumerate(cuts(d)):
                spot = mix_v.at[:, d, pl.ds(r0, rn), pl.ds(0, cols)]
                if not (inner(zz) or o == zz):
                    continue
                if o >= zz and inner(zz - 1):
                    crossing = last_g if far and zz == above else groups
                    sent(mix_v.at[pl.ds(0, crossing), d, pl.ds(r0, rn), pl.ds(0, cols)],
                         mx_dn.at[o, i])
                if o <= zz and inner(zz + 1):
                    sent(spot, mx_up.at[o, i])
                paired = last_g if far and zz == below and o >= above else groups
                sent(mix_v.at[pl.ds(0, paired), d, pl.ds(r0, rn), pl.ds(0, cols)], mx_ps.at[o, i])

    each_d(mix_sent)


def body(tokens, up_weight, gate_weight, group_gain, mix_weight, mix_bias, out_gain, out_weight):
    per, width = tokens.shape[1:]
    groups, gd = group_gain.shape
    rows, block = mix_weight.shape[1:]
    sp, dps = lax.axis_size("sp"), lax.axis_size("dp")
    zs = dps // CORES
    total = sp * per
    parts = groups
    halves = 1 if parts % 2 else 2
    bf, f32 = jnp.bfloat16, jnp.float32
    dma = pltpu.SemaphoreType.DMA
    hbm = pl.BlockSpec(memory_space=pltpu.HBM)
    vmem = pl.BlockSpec(memory_space=pltpu.VMEM)
    output = pl.pallas_call(
        functools.partial(fused_kernel, sp, zs),
        out_shape=pltpu.VMEM((per, width), bf),
        in_specs=[hbm, hbm, hbm, vmem, hbm, vmem, vmem, hbm],
        out_specs=vmem,
        scratch_shapes=[
            pltpu.VMEM((sp, per, width), bf),
            pltpu.VMEM((width, 2 * groups * gd), bf),
            pltpu.VMEM((groups, dps, rows, block), bf),
            pltpu.VMEM((parts, sp, groups * gd // parts, width), bf),
            pltpu.VMEM((groups, total, gd), f32),
            pltpu.VMEM((groups, total, gd), bf),
            pltpu.VMEM((groups, total, gd), bf),
            pltpu.VMEM((groups, block, gd), f32),
            pltpu.VMEM((groups, total // block, zs, CORES * rows, gd), bf),
            pltpu.VMEM((groups, total, gd), bf),
            pltpu.VMEM((sp, groups, per, gd), bf),
            pltpu.VMEM((parts, per, sp * groups * gd // parts), bf),
            pltpu.VMEM((per, gd), f32),
            pltpu.VMEM((per, width if parts > 1 else gd), f32),
            pltpu.VMEM((2, total if parts > 2 else 16, gd), bf),
            pltpu.VMEM((2, 2, total // block, CORES * rows if parts > 2 else 16, gd), bf),
            dma((4,)),
            dma((zs, 2)), dma((3,)), dma((1,)),
            dma((zs,)), dma((3,)), dma((1,)), dma((2,)),
            dma((sp,)), dma((sp, zs)), dma((1,)), dma((zs, halves)), dma((sp,)), dma((sp,)),
            dma((groups, zs)), dma((groups, zs)), dma((zs, 2)), dma((zs, 2)), dma((zs, 2)),
            dma((1,)), dma((sp, 2)), dma((2,)), dma((2, sp)),
            dma((1,)), dma((groups, zs)), dma((1,)), dma((parts, sp)),
            dma((2,)), dma((2,)), dma((2,)), dma((2,)),
        ],
        compiler_params=pltpu.CompilerParams(collective_id=0, has_side_effects=True, vmem_limit_bytes=65_000_000),
    )(tokens.reshape(per, width), up_weight, gate_weight, group_gain[:, None, :], mix_weight, mix_bias,
      out_gain[None, :], out_weight.reshape(sp, parts, groups * gd // parts, -1))
    return output.reshape(tokens.shape)


def solution(mesh):
    return jax.shard_map(
        body,
        mesh=mesh,
        in_specs=(
            P("dp", "sp", None),
            P("dp", None),
            P("dp", None),
            P("sp", None),
            P("sp", "dp", None),
            P("sp", None),
            P(),
            P(None, "dp"),
        ),
        out_specs=P("dp", "sp", None),
        check_vma=False,
    )
```

```python
import functools

import jax
import jax.numpy as jnp
from jax import lax
from jax.experimental import pallas as pl
from jax.experimental.pallas import tpu as pltpu
from jax.sharding import PartitionSpec as P

norm_eps = 1e-06
CORES = 2
LANES = 128
MESH = pl.DeviceIdType.MESH


def up_to(n, m):
    return -(-n // m) * m


def fused_kernel(
    sp, zs,
    tok_ref, up_ref, gate_ref, gain_ref, mix_ref, bias_ref, ogain_ref, outw_ref, out_ref,
    tok_v, ug_v, mix_v, outw_v, open_v, norm_v, other_v, bias_v, mixed_v, gated_v, held_v,
    normed_v, sums_v, part_v, far_v, far_m,
    load_sem, ug_line, ug_send, ug_pr, ow_line, ow_send, ow_pr, ow_own,
    pl_s, pl_r, p2_s, p2_r, pp_s, pp_r, mx_line, mx_pr, mx_up, mx_dn, mx_ps,
    tok_s, tok_r, v_s, v_r, ret_s, ret_r, ga_s, ga_r, fv_s, fv_r, fm_s, fm_r,
):
    me = lax.axis_index("sp")
    dp = lax.axis_index("dp")
    z, c = dp // CORES, lax.rem(dp, CORES)
    groups, dps, rows, block = mix_v.shape
    per, width = out_ref.shape
    gd = gain_ref.shape[2]
    chans = groups * gd
    depth, ncol = up_ref.shape[0], outw_ref.shape[3]
    total = sp * per
    blocks = total // block
    parts, _, pk, _ = outw_v.shape
    halves = 1 if parts % 2 else 2
    hp = parts // halves
    zr = CORES * rows
    half, dhalf = per // 2, depth // 2
    square = sp == 4
    far = zs == 4 and groups > 2
    below, above, last_g = zs // 2 - 1, zs // 2, groups - 1

    partner = {"dp": z * CORES + (1 - c)}

    def at_line(zz):
        return {"dp": zz * CORES + c}

    def around(r, sign):
        if square:
            y = lax.rem(me // 2 + r // 2, 2)
            x = lax.rem(lax.rem(me, 2) + r % 2, 2)
            return y * 2 + x
        return lax.rem(me + sign * r + sp, sp)

    def target(r):
        return around(r, 1)

    def source(r):
        return around(r, -1)

    def peer(r):
        return {"sp": target(r)}

    def inner(zz):
        return 0 < zz < zs - 1

    def mate(zz):
        return {0: 1, 1: 0, zs - 1: zs - 2, zs - 2: zs - 1}.get(zz)

    def remote(src, dst, send, recv, device):
        return pltpu.make_async_remote_copy(
            src_ref=src, dst_ref=dst, send_sem=send, recv_sem=recv,
            device_id=device, device_id_type=MESH)

    def sent(ref, sem):
        remote(ref, ref, sem, sem, partner).wait_send()

    def arrived(ref, sem):
        remote(ref, ref, sem, sem, partner).wait_recv()

    def each_z(fn, only=None):
        for zz in range(zs):
            if only is None or only(zz):
                pl.when(z == zz)(functools.partial(fn, zz))

    def each_d(fn, only=None):
        for zz in range(zs):
            if only is None or only(zz):
                for cc in range(CORES):
                    pl.when(dp == zz * CORES + cc)(functools.partial(fn, zz, cc))

    loads = {"ug": [], "tok": [], "ow": [], "mx": []}
    for g in range(groups):
        for t, ref in enumerate((up_ref, gate_ref)):
            cols = pl.ds(pl.multiple_of(me * chans + g * gd, LANES), gd)
            spot = 2 * g + t
            loads["ug"].append(pltpu.make_async_copy(
                ref.at[:, cols],
                ug_v.at[pl.ds(dp * depth, depth), pl.ds(spot * gd, gd)],
                load_sem.at[3]))
    loads["tok"].append(pltpu.make_async_copy(tok_ref, tok_v.at[me], load_sem.at[0]))
    own_cols = pl.ds(pl.multiple_of(dp * ncol, LANES), ncol)
    for p in range(parts):
        loads["ow"].append(pltpu.make_async_copy(
            outw_ref.at[:, p], outw_v.at[p, :, :, own_cols], load_sem.at[1]))
    loads["mx"].append(pltpu.make_async_copy(mix_ref, mix_v.at[:, dp], load_sem.at[2]))
    for kind in ("ug", "tok", "ow", "mx"):
        for load in loads[kind]:
            load.start()

    def loaded(ref, sem):
        pltpu.make_async_copy(ref, ref, sem).wait()

    barrier = pltpu.get_barrier_semaphore()

    def greet(zz):
        friends = [partner] + [peer(r) for r in range(1, sp)]
        if zz > 0:
            friends.append(at_line(zz - 1))
        if zz < zs - 1:
            friends.append(at_line(zz + 1))
        for friend in friends:
            pl.semaphore_signal(barrier, inc=1, device_id=friend, device_id_type=MESH)
        pl.semaphore_wait(barrier, len(friends))

    each_z(greet)

    def ug_piece(o, cc, h):
        return ug_v.at[pl.ds((o * CORES + cc) * depth + h * dhalf, dhalf), :]

    def ow_piece(s, o, cc):
        cols = pl.ds(pl.multiple_of((o * CORES + cc) * ncol, LANES), ncol)
        return outw_v.at[:, s, :, cols]

    def cuts(d):
        out, at, end = [], d * rows, (d + 1) * rows
        while at < end:
            top = min(end, (at // LANES + 1) * LANES)
            out.append((at - d * rows, top - at, min(block, up_to(top, LANES))))
            at = top
        return out

    def mx_bytes(d):
        size = sum(rn * cols for _, rn, cols in cuts(d))
        return open_v.at[0, pl.ds(0, size // gd // 2), :]

    def mx_piece(g, d, piece):
        r0, rn, cols = piece
        return mix_v.at[g, d, pl.ds(r0, rn), pl.ds(0, cols)]

    def ug_copies(zz, o, h):
        src, out = ug_piece(o, c, h), []
        if o >= zz and zz > 0:
            out.append(remote(src, src, ug_send.at[1], ug_line.at[o, h], at_line(zz - 1)))
        if o <= zz and zz < zs - 1:
            out.append(remote(src, src, ug_send.at[0], ug_line.at[o, h], at_line(zz + 1)))
        out.append(remote(src, src, ug_send.at[2], ug_pr.at[0], partner))
        return out

    def ow_down(zz, o):
        src = ow_piece(me, o, c)
        if o >= zz and zz > 0:
            return [remote(src, src, ow_send.at[1], ow_line.at[o], at_line(zz - 1))]
        return []

    def ow_rise(zz, o):
        src = ow_piece(me, o, c)
        if o <= zz and zz < zs - 1:
            return [remote(src, src, ow_send.at[0], ow_line.at[o], at_line(zz + 1))]
        return []

    def ow_pair(o):
        src = ow_piece(me, o, c)
        return [remote(src, src, ow_send.at[2], ow_pr.at[0], partner)]

    def ow_own_pair():
        src = outw_v.at[:, :, :, own_cols]
        return [remote(src, src, ow_own.at[0], ow_own.at[1], partner)]

    def ow_bytes(n):
        return outw_v.at[:, 0, :, pl.ds(0, n * ncol)]

    def mx_copies(zz, cc, g, o, way):
        out = []
        d = o * CORES + cc
        for i, piece in enumerate(cuts(d)):
            src = mx_piece(g, d, piece)
            if way == "dn" and o >= zz and inner(zz - 1):
                out.append(remote(src, src, mx_dn.at[o, i], mx_line.at[g, o], at_line(zz - 1)))
            if way == "up" and o <= zz and inner(zz + 1):
                out.append(remote(src, src, mx_up.at[o, i], mx_line.at[g, o], at_line(zz + 1)))
            if way == "pair" and (inner(zz) or o == zz):
                out.append(remote(src, src, mx_ps.at[o, i], mx_pr.at[g, o], partner))
        return out

    def go(copies):
        for copy in copies:
            copy.start()

    def own_mix(zz, way, low=0, high=groups):
        if far and zz == above and way == "dn":
            high = min(high, last_g)

        for cc in range(CORES):
            @pl.when(c == cc)
            def _():
                @pl.loop(low, high)
                def _(g):
                    go(mx_copies(zz, cc, g, zz, way))

    def ug_left(zz, way, k):
        far = zs - 1 - zz if way == "dn" else zz
        there = zz > 0 if way == "dn" else zz < zs - 1
        return there, max(0, far - k)

    held_back = max(1, groups - 1)

    def own_out(zz, way):
        go(ow_down(zz, zz) if way == "dn" else ow_rise(zz, zz))

    loaded(ug_v.at[pl.ds(dp * depth, depth), :], load_sem.at[3])

    def first_weights(zz):
        for h in range(2):
            go(ug_copies(zz, zz, h))

    each_z(first_weights)
    for load in loads["tok"]:
        load.wait()

    def tok_half(s, h):
        return tok_v.at[s, pl.ds(h * half, half), :]

    def tok_copy(s, r, h, r_there):
        return remote(tok_half(s, h), tok_half(s, h), tok_s.at[0], tok_r.at[r_there, h], peer(r))

    def tok_first():
        if square:
            return [tok_copy(me, 1, 0, 1), tok_copy(me, 2, 1, 2), tok_copy(me, 1, 1, 1), tok_copy(me, 2, 0, 2)]
        return [tok_copy(me, r, h, r) for r in range(1, sp) for h in range(2)]

    def tok_second():
        if square:
            return [tok_copy(source(1), 2, 0, 3), tok_copy(source(2), 1, 1, 3)]
        return []

    go(tok_first())
    loaded(outw_v.at[:, :, :, own_cols], load_sem.at[1])
    loads["mx"][0].wait()
    go(ow_own_pair())

    def first_rest(zz):
        for way in ("dn", "up"):
            there, left = ug_left(zz, way, 0)
            if there and left == 0:
                own_out(zz, way)
                own_mix(zz, way, 0, held_back if zz == zs - 1 else groups)
        own_mix(zz, "pair")

    each_z(first_rest)

    for g in range(groups):
        for t in range(block // LANES):
            spot = slice(t * LANES, (t + 1) * LANES)
            bias_v[g, spot, :] = jnp.broadcast_to(bias_ref[g:g + 1, spot], (gd, LANES)).T

    def take_ug(zz, k):
        for o in (zz + k, zz - k):
            if 0 <= o < zs:
                for h in range(2):
                    arrived(ug_piece(o, c, h), ug_line.at[o, h])
                    go(ug_copies(zz, o, h))
        for way in ("dn", "up"):
            there, left = ug_left(zz, way, k)
            before = ug_left(zz, way, k - 1)[1]
            if there and left == 0 and before > 0:
                own_out(zz, way)
                own_mix(zz, way, 0, 1)

    def take_out(zz, k):
        for o in (zz + k, zz - k):
            if 0 <= o < zs:
                arrived(ow_piece(me, o, c), ow_line.at[o])
                go(ow_down(zz, o) if o > zz else ow_rise(zz, o))
                go(ow_pair(o))
        for way in ("dn", "up"):
            there, left = ug_left(zz, way, k)
            before = ug_left(zz, way, k - 1)[1]
            if there and left == 0 and before > 0:
                own_mix(zz, way, 1, groups)

    def others(zz):
        return [o for k in range(1, zs) for o in (zz + k, zz - k) if 0 <= o < zs]

    def plane_first(o):
        src = ow_piece(me, o, c)
        reach = (1, 2) if square else range(1, sp)
        return [remote(src, src, pl_s.at[r], pl_r.at[r, o], peer(r)) for r in reach]

    def second_part(s, o, p):
        cols = pl.ds(pl.multiple_of((o * CORES + c) * ncol, LANES), ncol)
        return outw_v.at[pl.ds(p * hp, hp), s, :, cols]

    def plane_second(zz, o):
        if not square:
            return []
        units = [(x, p) for x in others(zz) for p in range(halves)]
        out = []
        for p in range(halves):
            via, to = (1, 2) if units.index((o, p)) < len(units) // 2 else (2, 1)
            src = second_part(source(via), o, p)
            out.append(remote(src, src, p2_s.at[0], p2_r.at[o, p], peer(to)))
        return out

    def plane_pair(r, o):
        src = ow_piece(source(r), o, c)
        return [remote(src, src, pp_s.at[r], pp_r.at[r], partner)]

    each_z(lambda zz: take_ug(zz, 1))
    if square:
        arrived(tok_half(source(1), 0), tok_r.at[1, 0])
        arrived(tok_half(source(2), 1), tok_r.at[2, 1])
    go(tok_second())

    def more_weights(zz):
        for k in range(2, zs):
            take_ug(zz, k)
        if inner(zz) and not square:
            for k in range(1, zs):
                take_out(zz, k)
            for o in others(zz):
                go(plane_first(o))

    each_z(more_weights)

    arrived(ug_v.at[pl.ds(0, zs * depth), :], ug_pr.at[0])

    def split(zz):
        return far and zz == below - 1

    def v_copies(zz, q):
        spot = pl.ds(pl.multiple_of(q * per, 16), per)
        ranges = ((last_g, 1), (0, last_g)) if split(zz) else ((0, groups),)
        out = []
        for i, (g0, gn) in enumerate(ranges):
            which = len(ranges) - 1 - i
            src, dst = (ref.at[pl.ds(g0, gn), spot, :] for ref in (norm_v, other_v))
            out.append(remote(src, dst, v_s.at[which], v_r.at[which, q], at_line(mate(zz))))
        return out

    def starts(q):
        return (q * per) % block

    def v_useful(end, q):
        return any(starts(q) < (o + 1) * zr for o in range(zs) if o != end) or block % per > 0

    def send_v(zz, s):
        for q in range(sp):
            if v_useful(zz, q):
                late_main = split(zz) and q >= sp // 2
                pl.when(s == q)(lambda q=q, n=1 if late_main else 2: go(v_copies(zz, q)[:n]))

    def far_send(i, ref):
        return remote(ref.at[last_g], far_v.at[i], fv_s.at[i], fv_r.at[i], at_line(above))

    def project(s):
        spot = pl.ds(pl.multiple_of(s * per, 16), per)

        @pl.loop(0, groups)
        def _(g):
            cols = pl.ds(pl.multiple_of(g * 2 * gd, 2 * gd), 2 * gd)
            both = jnp.dot(tok_v[s], ug_v[:, cols], preferred_element_type=jnp.float32)
            both = jax.nn.gelu(both.astype(jnp.bfloat16).astype(jnp.float32))
            open_v[g, spot, :] = both[:, :gd]
            act = both[:, gd:]
            act = act - jnp.mean(act, axis=-1, keepdims=True)
            spread = jnp.mean(act * act, axis=-1, keepdims=True)
            norm_v[g, spot, :] = (
                act * lax.rsqrt(spread + norm_eps) * gain_ref[g]
            ).astype(jnp.bfloat16)

        each_z(lambda zz: send_v(zz, s), lambda zz: not inner(zz))

    def out_events(zz, ks):
        for k in ks:
            take_out(zz, k)
            for o in (zz + k, zz - k):
                if 0 <= o < zs:
                    go(plane_first(o))

    if square:
        def in_order(i):
            place = jnp.where(me == sp - 1, 1 - i, i) if i < 2 else i
            return jnp.where((z == 0) | (z == zs - 1), source(place), i)

        for r in range(sp):
            turn = in_order(r)
            for h in range(2):
                @pl.when((turn > 0) & (turn != 1 + h))
                def _():
                    arrived(tok_half(source(turn), h), tok_r.at[turn, h])
            project(source(turn))
            if r == 1 and held_back < groups:
                each_z(lambda zz: own_mix(zz, "dn", held_back, groups), lambda zz: zz == zs - 1)
            if r == sp - 1:
                for q in range(sp // 2, sp):
                    each_z(lambda zz: go(v_copies(zz, q)[1:]), split)

            def events(zz, r=r):
                first = r + 1 if inner(zz) else r
                ks = range(first, zs if r == sp - 1 else first + 1)
                out_events(zz, [k for k in ks if 0 < k < zs])

            each_z(events)
    else:
        @pl.loop(0, sp)
        def _(r):
            @pl.when(r > 0)
            def _():
                for h in range(2):
                    arrived(tok_half(source(r), h), tok_r.at[r, h])

            project(source(r))

        each_z(lambda zz: out_events(zz, range(1, zs)), lambda zz: not inner(zz))

    def take_mix(zz, cc, g, o, onward=True):
        d = o * CORES + cc
        arrived(mx_bytes(d), mx_line.at[g, o])
        if onward:
            go(mx_copies(zz, cc, g, o, "dn" if o > zz else "up"))
        go(mx_copies(zz, cc, g, o, "pair"))

    def passed_on(zz, o):
        return abs(o - zz) == 1 and inner(zz - 1 if o > zz else zz + 1)

    def late(zz, o):
        return zz == zs - 2 and o == zs - 1

    def near_mix(zz, cc):
        for o in (zz + 1, zz - 1):
            if passed_on(zz, o):
                @pl.loop(0, held_back if late(zz, o) else groups)
                def _(g):
                    take_mix(zz, cc, g, o)

    def late_mix(zz, cc):
        @pl.loop(held_back, groups)
        def _(g):
            take_mix(zz, cc, g, zz + 1, not far)

    each_d(near_mix, inner)
    if far:
        each_z(lambda zz: far_send(0, norm_v).start(), lambda zz: zz == below)

    def ready_at(q):
        if block % per:
            return zs - 1
        return (((q + 1) * per - 1) % block) // zr

    def needs(o):
        return min(block, up_to((o + 1) * zr, LANES))

    def first_need(zz, q):
        if not v_useful(mate(zz), q):
            return None
        return next(o for o in range(zs) if o != mate(zz) and (block % per or starts(q) < (o + 1) * zr))

    def with_mate(zz, o):
        return inner(zz) and mate(zz) is not None and mate(zz) != o

    def alone(zz, o):
        return zz == o if not inner(zz) else not with_mate(zz, o)

    def gated_copy(g, q):
        return remote(gated_v.at[g, pl.ds(q * per, per), :], held_v.at[me, g],
                      ga_s.at[0], ga_r.at[g, me], {"sp": q})

    def ret_copy(zz, g, o):
        spot = mixed_v.at[g, :, o]
        return remote(spot, spot, ret_s.at[0], ret_r.at[g, o], at_line(mate(zz)))

    def hand_over(g, o):
        for q in range(sp):
            if ready_at(q) == o:
                @pl.when(me == q)
                def _():
                    held_v[q, g] = gated_v[g, pl.ds(q * per, per), :]

                @pl.when(me != q)
                def _():
                    gated_copy(g, q).start()

    def one_of(zs_in):
        return functools.reduce(jnp.logical_or, [z == zz for zz in zs_in])

    def unit(o, low=0, high=groups, only=None, but=()):
        lo = o * zr
        base, top = lo // LANES * LANES, needs(o)

        def wait_v(zz):
            apart = split(mate(zz))
            for q in range(sp):
                if first_need(zz, q) == o:
                    rows_of = pl.ds(q * per, per)
                    main = pl.ds(0, last_g if apart else groups)
                    arrived(other_v.at[main, rows_of, :], v_r.at[0, q])
                    if apart and o < above:
                        arrived(other_v.at[pl.ds(last_g, 1), rows_of, :], v_r.at[1, q])

        if low == 0:
            each_z(wait_v, lambda zz: with_mate(zz, o) and zz not in but and only in (None, zz))

        def mix(members, paired):
            def rows_from_line(zz, cc):
                @pl.loop(low, high)
                def _(g):
                    take_mix(zz, cc, g, o)

            each_d(rows_from_line, lambda zz: zz in members and o != zz and not passed_on(zz, o))

            @pl.loop(low, high)
            def _(g):
                def rows_in(zz, cc):
                    if not (far and zz == above and o >= above and low == last_g):
                        arrived(mx_bytes(o * CORES + 1 - cc), mx_pr.at[g, o])

                def values(at, end, spare=0):
                    own = norm_v[g, at:end, :]
                    if not paired:
                        return own
                    other = other_v[g, at:end - spare, :]
                    if spare:
                        zeros = jnp.zeros((spare, gd), jnp.bfloat16)
                        other = jnp.concatenate([other, zeros], axis=0)
                    return jnp.concatenate([own, other], axis=1)

                each_d(rows_in, lambda zz: zz in members)
                corner = mix_v[g, o * CORES:(o + 1) * CORES, :, base:top].reshape(zr, top - base)
                keep = lax.broadcasted_iota(jnp.int32, corner.shape, 0) + (lo - base) >= (
                    lax.broadcasted_iota(jnp.int32, corner.shape, 1))
                corner = jnp.where(keep, corner.astype(jnp.float32), 0.0).astype(jnp.bfloat16)
                bias = bias_v[g, lo:lo + zr, :]
                for b in range(blocks):
                    at = b * block
                    mixed = jnp.dot(corner, values(at + base, at + top, top - lo - zr),
                                    preferred_element_type=jnp.float32)
                    if base > 0:
                        left = mix_v[g, o * CORES:(o + 1) * CORES, :, :base].reshape(zr, base)
                        mixed += jnp.dot(left, values(at, at + base),
                                         preferred_element_type=jnp.float32)
                    spot = slice(at + lo, at + lo + zr)
                    if paired:
                        mixed_v[g, b, o] = (mixed[:, gd:] + bias).astype(jnp.bfloat16)
                    gated_v[g, spot, :] = (
                        open_v[g, spot, :] * (mixed[:, :gd] + bias)).astype(jnp.bfloat16)
                if paired:
                    each_z(lambda zz: ret_copy(zz, g, o).start(), lambda zz: zz in members)
                hand_over(g, o)

        for paired, test in ((True, with_mate), (False, alone)):
            members = [zz for zz in range(zs) if test(zz, o) and zz not in but and only in (None, zz)]
            if members:
                pl.when(one_of(members))(functools.partial(mix, members, paired))

        if only is not None:
            return

        waiting = [zz for zz in (0, zs - 1) if zz != o and zz not in but]
        if not waiting:
            return

        @pl.when(one_of(waiting))
        def _():
            @pl.loop(low, high)
            def _(g):
                arrived(mixed_v.at[g, :, o], ret_r.at[g, o])
                for b in range(blocks):
                    spot = slice(b * block + lo, b * block + lo + zr)
                    gated_v[g, spot, :] = (
                        open_v[g, spot, :] * mixed_v[g, b, o].astype(jnp.float32)
                    ).astype(jnp.bfloat16)
                hand_over(g, o)

    def plane_round(zz):
        for o in others(zz):
            for r in range(1, sp):
                if not (square and r == 3):
                    arrived(ow_piece(source(r), o, c), pl_r.at[r, o])
            go(plane_second(zz, o))
            for r in range(1, sp):
                if not (square and r == 3):
                    go(plane_pair(r, o))

    def plane_end(zz):
        for o in others(zz):
            for p in range(halves):
                arrived(second_part(source(3), o, p), p2_r.at[o, p])
            go(plane_pair(3, o))

    def far_forward(zz):
        for q in range(sp):
            if first_need(zz, q) >= above:
                arrived(other_v.at[pl.ds(last_g, 1), pl.ds(q * per, per), :], v_r.at[1, q])
        far_send(1, other_v).start()

    def far_unit(i):
        o = above + i
        lo, top = o * zr, needs(o)
        base = lo // LANES * LANES
        rows_of = slice(o * CORES, (o + 1) * CORES)
        corner = mix_v[last_g, rows_of, :, base:top].reshape(zr, top - base)
        keep = lax.broadcasted_iota(jnp.int32, corner.shape, 0) + (lo - base) >= (
            lax.broadcasted_iota(jnp.int32, corner.shape, 1))
        corner = jnp.where(keep, corner.astype(jnp.float32), 0.0).astype(jnp.bfloat16)
        left = mix_v[last_g, rows_of, :, :base].reshape(zr, base)
        bias = bias_v[last_g, lo:lo + zr, :]

        def values(at, end):
            return jnp.concatenate([far_v[0, at:end, :], far_v[1, at:end, :]], axis=1)

        for b in range(blocks):
            at = b * block
            mixed = jnp.dot(left, values(at, at + base), preferred_element_type=jnp.float32)
            mixed += jnp.dot(corner, values(at + base, at + top), preferred_element_type=jnp.float32)
            for n in range(2):
                far_m[n, i, b] = (mixed[:, n * gd:(n + 1) * gd] + bias).astype(jnp.bfloat16)

    def far_back(i):
        spot = far_m.at[:, i]
        return remote(spot, spot, fm_s.at[i], fm_r.at[i], at_line(below))

    def far_above(zz):
        for i in range(2):
            arrived(far_v.at[i], fv_r.at[i])
        for cc in range(CORES):
            @pl.when(c == cc)
            def _():
                for o in (above, zs - 1):
                    arrived(mx_bytes(o * CORES + 1 - cc), mx_pr.at[last_g, o])
        for i in (1, 0):
            far_unit(i)
            far_back(i).start()

    def far_ret(i):
        return remote(far_m.at[1, i], mixed_v.at[last_g, :, above + i],
                      ret_s.at[0], ret_r.at[last_g, above + i], at_line(below - 1))

    def far_below(zz):
        for i in (1, 0):
            o = above + i
            if zz == below:
                arrived(far_m.at[:, i], fm_r.at[i])
                far_ret(i).start()
            else:
                arrived(mixed_v.at[last_g, :, o], ret_r.at[last_g, o])
            for b in range(blocks):
                spot = slice(b * block + o * zr, b * block + (o + 1) * zr)
                mixed = far_m[0, i, b] if zz == below else mixed_v[last_g, b, o]
                gated_v[last_g, spot, :] = (
                    open_v[last_g, spot, :] * mixed.astype(jnp.float32)).astype(jnp.bfloat16)
            hand_over(last_g, o)

    ends, insides = (0, zs - 1), tuple(range(1, zs - 1))
    unit(zs - 1, 0, held_back, only=zs - 2)
    for o in range(zs // 2):
        unit(o, but=ends)
    if far:
        each_z(far_forward, lambda zz: zz == below)
    each_z(plane_round)

    unit(zs - 1, only=zs - 1)
    lower = (below - 1, below)
    for o in range(zs - 1):
        if o < zs // 2:
            unit(o, but=insides)
        elif far and o == above:
            each_d(late_mix, lambda zz: late(zz, zz + 1))
            each_z(far_above, lambda zz: zz == above)
            unit(o, 0, last_g)
            unit(o, last_g, groups, but=lower)
        else:
            unit(o)
    if held_back < groups and not far:
        each_d(late_mix, lambda zz: late(zz, zz + 1))

    def gather_part(g, first):
        for s in range(sp):
            @pl.when(me != s)
            def _():
                arrived(held_v.at[s, g], ga_r.at[g, s])
        squares = jnp.zeros((per, gd), jnp.float32)
        for s in range(sp):
            value = held_v[s, g].astype(jnp.float32)
            squares += value * value
            cols = slice(s * chans + g * gd, s * chans + (g + 1) * gd)
            normed_v[g, :, s * pk:(s + 1) * pk] = (value * ogain_ref[:, cols]).astype(jnp.bfloat16)
        sums_v[...] = squares if first else sums_v[...] + squares

    step = 2 * ncol if width % (2 * ncol) == 0 else ncol

    def part_dot(p, cols):
        return jnp.dot(normed_v[p], outw_v[p, :, :, cols].reshape(sp * pk, step),
                       preferred_element_type=jnp.float32)

    def weights_here():
        arrived(outw_v.at[:, :, :, own_cols], ow_own.at[1])
        arrived(ow_bytes(zs - 1), ow_pr.at[0])
        for r in range(1, sp):
            arrived(ow_bytes(zs - 1), pp_r.at[r])

    started = []

    def add_parts(which):
        for g in which:
            gather_part(g, not started)
            started.append(g)

        @pl.loop(0, width // step)
        def _(t):
            cols = pl.ds(pl.multiple_of(t * step, LANES), step)
            more = sum(part_dot(p, cols) for p in which)
            part_v[:, cols] = more if len(started) == len(which) else part_v[:, cols] + more

    done = (zs - 1, zs - 2)
    if far:
        unit(zs - 1, 0, last_g - 1, but=done)
        early = (me < sp - 1) & ((z == 0) | (z == zs - 1))

        def first_parts():
            started.clear()
            weights_here()
            add_parts(range(last_g - 1))

        if square:
            each_z(plane_end)
        pl.when(early)(first_parts)
        each_z(far_below, lambda zz: zz in lower)
        unit(zs - 1, last_g - 1, last_g, but=done)
        unit(zs - 1, last_g, groups, but=lower + (zs - 1,))
        pl.when(jnp.logical_not(early))(first_parts)
        add_parts([last_g])
        final = last_g - 1
    elif groups > 1:
        if square:
            each_z(plane_end)
        weights_here()
        unit(zs - 1, 0, last_g, but=done)
        add_parts(range(last_g))
        unit(zs - 1, last_g, groups, but=(zs - 1,))
        final = last_g
    else:
        if square:
            each_z(plane_end)
        weights_here()
        unit(zs - 1, but=done)
        final = 0
    gather_part(final, not started)
    scale = lax.rsqrt(jnp.sum(sums_v[...], axis=-1, keepdims=True) / (sp * chans) + norm_eps)

    @pl.loop(0, width // step)
    def _(t):
        cols = pl.ds(pl.multiple_of(t * step, LANES), step)
        last = part_dot(final, cols)
        if started:
            last += part_v[:, cols]
        out_ref[:, cols] = (last * scale).astype(jnp.bfloat16)

    sent(tok_v.at[pl.ds(0, sp - 1)], tok_s.at[0])
    sent(outw_v.at[:, :, :, own_cols], ow_own.at[0])
    for r in range(1, sp):
        if not (square and r == 3):
            sent(ow_bytes(zs - 1), pl_s.at[r])
        sent(ow_bytes(zs - 1), pp_s.at[r])
    if square:
        sent(ow_bytes(zs - 1), p2_s.at[0])
    sent(ow_bytes(zs - 1), ow_send.at[2])
    sent(ug_v.at[pl.ds(0, zs * depth), :], ug_send.at[2])
    sent(held_v.at[pl.ds(0, sp - 1)], ga_s.at[0])

    def line_sent(zz):
        for n, way in ((zz + 1 if zz < zs - 1 else 0, 0), (zs - zz if zz > 0 else 0, 1)):
            if n:
                sent(ug_v.at[pl.ds(0, n * depth), :], ug_send.at[way])
                sent(ow_bytes(n), ow_send.at[way])
        if not inner(zz):
            n = sum(v_useful(zz, q) for q in range(sp))
            main = pl.ds(0, last_g if split(zz) else groups)
            sent(norm_v.at[main, pl.ds(0, n * per), :], v_s.at[0])
            if split(zz):
                sent(norm_v.at[pl.ds(0, 1), pl.ds(0, n * per), :], v_s.at[1])
        elif mate(zz) is not None:
            n = sum(with_mate(zz, o) for o in range(zs))
            sent(mixed_v.at[:, :, pl.ds(0, n)], ret_s.at[0])
        for i in range(2):
            if far and zz == below:
                sent(far_v.at[i], fv_s.at[i])
            if far and zz == above:
                sent(far_m.at[:, i], fm_s.at[i])

    each_z(line_sent)

    def mix_sent(zz, cc):
        for o in range(zs):
            d = o * CORES + cc
            for i, (r0, rn, cols) in enumerate(cuts(d)):
                spot = mix_v.at[:, d, pl.ds(r0, rn), pl.ds(0, cols)]
                if not (inner(zz) or o == zz):
                    continue
                if o >= zz and inner(zz - 1):
                    crossing = last_g if far and zz == above else groups
                    sent(mix_v.at[pl.ds(0, crossing), d, pl.ds(r0, rn), pl.ds(0, cols)],
                         mx_dn.at[o, i])
                if o <= zz and inner(zz + 1):
                    sent(spot, mx_up.at[o, i])
                paired = last_g if far and zz == below and o >= above else groups
                sent(mix_v.at[pl.ds(0, paired), d, pl.ds(r0, rn), pl.ds(0, cols)], mx_ps.at[o, i])

    each_d(mix_sent)


def body(tokens, up_weight, gate_weight, group_gain, mix_weight, mix_bias, out_gain, out_weight):
    per, width = tokens.shape[1:]
    groups, gd = group_gain.shape
    rows, block = mix_weight.shape[1:]
    sp, dps = lax.axis_size("sp"), lax.axis_size("dp")
    zs = dps // CORES
    total = sp * per
    parts = groups
    halves = 1 if parts % 2 else 2
    bf, f32 = jnp.bfloat16, jnp.float32
    dma = pltpu.SemaphoreType.DMA
    hbm = pl.BlockSpec(memory_space=pltpu.HBM)
    vmem = pl.BlockSpec(memory_space=pltpu.VMEM)
    output = pl.pallas_call(
        functools.partial(fused_kernel, sp, zs),
        out_shape=pltpu.VMEM((per, width), bf),
        in_specs=[hbm, hbm, hbm, vmem, hbm, vmem, vmem, hbm],
        out_specs=vmem,
        scratch_shapes=[
            pltpu.VMEM((sp, per, width), bf),
            pltpu.VMEM((width, 2 * groups * gd), bf),
            pltpu.VMEM((groups, dps, rows, block), bf),
            pltpu.VMEM((parts, sp, groups * gd // parts, width), bf),
            pltpu.VMEM((groups, total, gd), f32),
            pltpu.VMEM((groups, total, gd), bf),
            pltpu.VMEM((groups, total, gd), bf),
            pltpu.VMEM((groups, block, gd), f32),
            pltpu.VMEM((groups, total // block, zs, CORES * rows, gd), bf),
            pltpu.VMEM((groups, total, gd), bf),
            pltpu.VMEM((sp, groups, per, gd), bf),
            pltpu.VMEM((parts, per, sp * groups * gd // parts), bf),
            pltpu.VMEM((per, gd), f32),
            pltpu.VMEM((per, width if parts > 1 else gd), f32),
            pltpu.VMEM((2, total if parts > 2 else 16, gd), bf),
            pltpu.VMEM((2, 2, total // block, CORES * rows if parts > 2 else 16, gd), bf),
            dma((4,)),
            dma((zs, 2)), dma((3,)), dma((1,)),
            dma((zs,)), dma((3,)), dma((1,)), dma((2,)),
            dma((sp,)), dma((sp, zs)), dma((1,)), dma((zs, halves)), dma((sp,)), dma((sp,)),
            dma((groups, zs)), dma((groups, zs)), dma((zs, 2)), dma((zs, 2)), dma((zs, 2)),
            dma((1,)), dma((sp, 2)), dma((2,)), dma((2, sp)),
            dma((1,)), dma((groups, zs)), dma((1,)), dma((parts, sp)),
            dma((2,)), dma((2,)), dma((2,)), dma((2,)),
        ],
        compiler_params=pltpu.CompilerParams(collective_id=0, has_side_effects=True, vmem_limit_bytes=65_000_000),
    )(tokens.reshape(per, width), up_weight, gate_weight, group_gain[:, None, :], mix_weight, mix_bias,
      out_gain[None, :], out_weight.reshape(sp, parts, groups * gd // parts, -1))
    return output.reshape(tokens.shape)


def solution(mesh):
    return jax.shard_map(
        body,
        mesh=mesh,
        in_specs=(
            P("dp", "sp", None),
            P("dp", None),
            P("dp", None),
            P("sp", None),
            P("sp", "dp", None),
            P("sp", None),
            P(),
            P(None, "dp"),
        ),
        out_specs=P("dp", "sp", None),
        check_vma=False,
    )
```

```python
import functools

import jax
import jax.numpy as jnp
from jax import lax
from jax.experimental import pallas as pl
from jax.experimental.pallas import tpu as pltpu
from jax.sharding import PartitionSpec as P

norm_eps = 1e-06
CORES = 2
LANES = 128
MESH = pl.DeviceIdType.MESH


def up_to(n, m):
    return -(-n // m) * m


def fused_kernel(
    sp, zs,
    tok_ref, up_ref, gate_ref, gain_ref, mix_ref, bias_ref, ogain_ref, outw_ref, out_ref,
    tok_v, ug_v, mix_v, outw_v, open_v, norm_v, other_v, bias_v, mixed_v, gated_v, held_v,
    normed_v, sums_v, part_v, far_v, far_m,
    load_sem, ug_line, ug_send, ug_pr, ow_line, ow_send, ow_pr, ow_own,
    pl_s, pl_r, p2_s, p2_r, pp_s, pp_r, mx_line, mx_pr, mx_up, mx_dn, mx_ps,
    tok_s, tok_r, v_s, v_r, ret_s, ret_r, ga_s, ga_r, fv_s, fv_r, fm_s, fm_r,
):
    me = lax.axis_index("sp")
    dp = lax.axis_index("dp")
    z, c = dp // CORES, lax.rem(dp, CORES)
    groups, dps, rows, block = mix_v.shape
    per, width = out_ref.shape
    gd = gain_ref.shape[2]
    chans = groups * gd
    depth, ncol = up_ref.shape[0], outw_ref.shape[3]
    total = sp * per
    blocks = total // block
    parts, _, pk, _ = outw_v.shape
    halves = 1 if parts % 2 else 2
    hp = parts // halves
    zr = CORES * rows
    half, dhalf = per // 2, depth // 2
    square = sp == 4
    far = zs == 4 and groups > 2
    below, above, last_g = zs // 2 - 1, zs // 2, groups - 1

    partner = {"dp": z * CORES + (1 - c)}

    def at_line(zz):
        return {"dp": zz * CORES + c}

    def around(r, sign):
        if square:
            y = lax.rem(me // 2 + r // 2, 2)
            x = lax.rem(lax.rem(me, 2) + r % 2, 2)
            return y * 2 + x
        return lax.rem(me + sign * r + sp, sp)

    def target(r):
        return around(r, 1)

    def source(r):
        return around(r, -1)

    def peer(r):
        return {"sp": target(r)}

    def inner(zz):
        return 0 < zz < zs - 1

    def mate(zz):
        return {0: 1, 1: 0, zs - 1: zs - 2, zs - 2: zs - 1}.get(zz)

    def remote(src, dst, send, recv, device):
        return pltpu.make_async_remote_copy(
            src_ref=src, dst_ref=dst, send_sem=send, recv_sem=recv,
            device_id=device, device_id_type=MESH)

    def sent(ref, sem):
        remote(ref, ref, sem, sem, partner).wait_send()

    def arrived(ref, sem):
        remote(ref, ref, sem, sem, partner).wait_recv()

    def each_z(fn, only=None):
        for zz in range(zs):
            if only is None or only(zz):
                pl.when(z == zz)(functools.partial(fn, zz))

    def each_d(fn, only=None):
        for zz in range(zs):
            if only is None or only(zz):
                for cc in range(CORES):
                    pl.when(dp == zz * CORES + cc)(functools.partial(fn, zz, cc))

    loads = {"ug": [], "tok": [], "ow": [], "mx": []}
    for g in range(groups):
        for t, ref in enumerate((up_ref, gate_ref)):
            cols = pl.ds(pl.multiple_of(me * chans + g * gd, LANES), gd)
            spot = 2 * g + t
            loads["ug"].append(pltpu.make_async_copy(
                ref.at[:, cols],
                ug_v.at[pl.ds(dp * depth, depth), pl.ds(spot * gd, gd)],
                load_sem.at[3]))
    loads["tok"].append(pltpu.make_async_copy(tok_ref, tok_v.at[me], load_sem.at[0]))
    own_cols = pl.ds(pl.multiple_of(dp * ncol, LANES), ncol)
    for p in range(parts):
        loads["ow"].append(pltpu.make_async_copy(
            outw_ref.at[:, p], outw_v.at[p, :, :, own_cols], load_sem.at[1]))
    loads["mx"].append(pltpu.make_async_copy(mix_ref, mix_v.at[:, dp], load_sem.at[2]))
    for kind in ("ug", "tok", "ow", "mx"):
        for load in loads[kind]:
            load.start()

    def loaded(ref, sem):
        pltpu.make_async_copy(ref, ref, sem).wait()

    barrier = pltpu.get_barrier_semaphore()

    def greet(zz):
        friends = [partner] + [peer(r) for r in range(1, sp)]
        if zz > 0:
            friends.append(at_line(zz - 1))
        if zz < zs - 1:
            friends.append(at_line(zz + 1))
        for friend in friends:
            pl.semaphore_signal(barrier, inc=1, device_id=friend, device_id_type=MESH)
        pl.semaphore_wait(barrier, len(friends))

    each_z(greet)

    def ug_piece(o, cc, h):
        return ug_v.at[pl.ds((o * CORES + cc) * depth + h * dhalf, dhalf), :]

    def ow_piece(s, o, cc):
        cols = pl.ds(pl.multiple_of((o * CORES + cc) * ncol, LANES), ncol)
        return outw_v.at[:, s, :, cols]

    def cuts(d):
        out, at, end = [], d * rows, (d + 1) * rows
        while at < end:
            top = min(end, (at // LANES + 1) * LANES)
            out.append((at - d * rows, top - at, min(block, up_to(top, LANES))))
            at = top
        return out

    def mx_bytes(d):
        size = sum(rn * cols for _, rn, cols in cuts(d))
        return open_v.at[0, pl.ds(0, size // gd // 2), :]

    def mx_piece(g, d, piece):
        r0, rn, cols = piece
        return mix_v.at[g, d, pl.ds(r0, rn), pl.ds(0, cols)]

    def ug_copies(zz, o, h):
        src, out = ug_piece(o, c, h), []
        if o >= zz and zz > 0:
            out.append(remote(src, src, ug_send.at[1], ug_line.at[o, h], at_line(zz - 1)))
        if o <= zz and zz < zs - 1:
            out.append(remote(src, src, ug_send.at[0], ug_line.at[o, h], at_line(zz + 1)))
        out.append(remote(src, src, ug_send.at[2], ug_pr.at[0], partner))
        return out

    def ow_down(zz, o):
        src = ow_piece(me, o, c)
        if o >= zz and zz > 0:
            return [remote(src, src, ow_send.at[1], ow_line.at[o], at_line(zz - 1))]
        return []

    def ow_rise(zz, o):
        src = ow_piece(me, o, c)
        if o <= zz and zz < zs - 1:
            return [remote(src, src, ow_send.at[0], ow_line.at[o], at_line(zz + 1))]
        return []

    def ow_pair(o):
        src = ow_piece(me, o, c)
        return [remote(src, src, ow_send.at[2], ow_pr.at[0], partner)]

    def ow_own_pair():
        src = outw_v.at[:, :, :, own_cols]
        return [remote(src, src, ow_own.at[0], ow_own.at[1], partner)]

    def ow_bytes(n):
        return outw_v.at[:, 0, :, pl.ds(0, n * ncol)]

    def mx_copies(zz, cc, g, o, way):
        out = []
        d = o * CORES + cc
        for i, piece in enumerate(cuts(d)):
            src = mx_piece(g, d, piece)
            if way == "dn" and o >= zz and inner(zz - 1):
                out.append(remote(src, src, mx_dn.at[o, i], mx_line.at[g, o], at_line(zz - 1)))
            if way == "up" and o <= zz and inner(zz + 1):
                out.append(remote(src, src, mx_up.at[o, i], mx_line.at[g, o], at_line(zz + 1)))
            if way == "pair" and (inner(zz) or o == zz):
                out.append(remote(src, src, mx_ps.at[o, i], mx_pr.at[g, o], partner))
        return out

    def go(copies):
        for copy in copies:
            copy.start()

    def own_mix(zz, way, low=0, high=groups):
        if far and zz == above and way == "dn":
            high = min(high, last_g)

        for cc in range(CORES):
            @pl.when(c == cc)
            def _():
                @pl.loop(low, high)
                def _(g):
                    go(mx_copies(zz, cc, g, zz, way))

    def ug_left(zz, way, k):
        far = zs - 1 - zz if way == "dn" else zz
        there = zz > 0 if way == "dn" else zz < zs - 1
        return there, max(0, far - k)

    held_back = max(1, groups - 1)

    def own_out(zz, way):
        go(ow_down(zz, zz) if way == "dn" else ow_rise(zz, zz))

    loaded(ug_v.at[pl.ds(dp * depth, depth), :], load_sem.at[3])

    def first_weights(zz):
        for h in range(2):
            go(ug_copies(zz, zz, h))

    each_z(first_weights)
    for load in loads["tok"]:
        load.wait()

    def tok_half(s, h):
        return tok_v.at[s, pl.ds(h * half, half), :]

    def tok_copy(s, r, h, r_there):
        return remote(tok_half(s, h), tok_half(s, h), tok_s.at[0], tok_r.at[r_there, h], peer(r))

    def tok_first():
        if square:
            return [tok_copy(me, 1, 0, 1), tok_copy(me, 2, 1, 2), tok_copy(me, 1, 1, 1), tok_copy(me, 2, 0, 2)]
        return [tok_copy(me, r, h, r) for r in range(1, sp) for h in range(2)]

    def tok_second():
        if square:
            return [tok_copy(source(1), 2, 0, 3), tok_copy(source(2), 1, 1, 3)]
        return []

    go(tok_first())
    loaded(outw_v.at[:, :, :, own_cols], load_sem.at[1])
    loads["mx"][0].wait()
    go(ow_own_pair())

    def first_rest(zz):
        for way in ("dn", "up"):
            there, left = ug_left(zz, way, 0)
            if there and left == 0:
                own_out(zz, way)
                own_mix(zz, way, 0, held_back if zz == zs - 1 else groups)
        own_mix(zz, "pair")

    each_z(first_rest)

    for g in range(groups):
        for t in range(block // LANES):
            spot = slice(t * LANES, (t + 1) * LANES)
            bias_v[g, spot, :] = jnp.broadcast_to(bias_ref[g:g + 1, spot], (gd, LANES)).T

    def take_ug(zz, k):
        for o in (zz + k, zz - k):
            if 0 <= o < zs:
                for h in range(2):
                    arrived(ug_piece(o, c, h), ug_line.at[o, h])
                    go(ug_copies(zz, o, h))
        for way in ("dn", "up"):
            there, left = ug_left(zz, way, k)
            before = ug_left(zz, way, k - 1)[1]
            if there and left == 0 and before > 0:
                own_out(zz, way)
                own_mix(zz, way, 0, 1)

    def take_out(zz, k):
        for o in (zz + k, zz - k):
            if 0 <= o < zs:
                arrived(ow_piece(me, o, c), ow_line.at[o])
                go(ow_down(zz, o) if o > zz else ow_rise(zz, o))
                go(ow_pair(o))
        for way in ("dn", "up"):
            there, left = ug_left(zz, way, k)
            before = ug_left(zz, way, k - 1)[1]
            if there and left == 0 and before > 0:
                own_mix(zz, way, 1, groups)

    def others(zz):
        return [o for k in range(1, zs) for o in (zz + k, zz - k) if 0 <= o < zs]

    def plane_first(o):
        src = ow_piece(me, o, c)
        reach = (1, 2) if square else range(1, sp)
        return [remote(src, src, pl_s.at[r], pl_r.at[r, o], peer(r)) for r in reach]

    def second_part(s, o, p):
        cols = pl.ds(pl.multiple_of((o * CORES + c) * ncol, LANES), ncol)
        return outw_v.at[pl.ds(p * hp, hp), s, :, cols]

    def plane_second(zz, o):
        if not square:
            return []
        units = [(x, p) for x in others(zz) for p in range(halves)]
        out = []
        for p in range(halves):
            via, to = (1, 2) if units.index((o, p)) < len(units) // 2 else (2, 1)
            src = second_part(source(via), o, p)
            out.append(remote(src, src, p2_s.at[0], p2_r.at[o, p], peer(to)))
        return out

    def plane_pair(r, o):
        src = ow_piece(source(r), o, c)
        return [remote(src, src, pp_s.at[r], pp_r.at[r], partner)]

    each_z(lambda zz: take_ug(zz, 1))
    if square:
        arrived(tok_half(source(1), 0), tok_r.at[1, 0])
        arrived(tok_half(source(2), 1), tok_r.at[2, 1])
    go(tok_second())

    def more_weights(zz):
        for k in range(2, zs):
            take_ug(zz, k)
        if inner(zz) and not square:
            for k in range(1, zs):
                take_out(zz, k)
            for o in others(zz):
                go(plane_first(o))

    each_z(more_weights)

    arrived(ug_v.at[pl.ds(0, zs * depth), :], ug_pr.at[0])

    def split(zz):
        return far and zz == below - 1

    def v_copies(zz, q):
        spot = pl.ds(pl.multiple_of(q * per, 16), per)
        ranges = ((last_g, 1), (0, last_g)) if split(zz) else ((0, groups),)
        out = []
        for i, (g0, gn) in enumerate(ranges):
            which = len(ranges) - 1 - i
            src, dst = (ref.at[pl.ds(g0, gn), spot, :] for ref in (norm_v, other_v))
            out.append(remote(src, dst, v_s.at[which], v_r.at[which, q], at_line(mate(zz))))
        return out

    def starts(q):
        return (q * per) % block

    def v_useful(end, q):
        return any(starts(q) < (o + 1) * zr for o in range(zs) if o != end) or block % per > 0

    def send_v(zz, s):
        for q in range(sp):
            if v_useful(zz, q):
                late_main = split(zz) and q >= sp // 2
                pl.when(s == q)(lambda q=q, n=1 if late_main else 2: go(v_copies(zz, q)[:n]))

    def far_send(i, ref):
        return remote(ref.at[last_g], far_v.at[i], fv_s.at[i], fv_r.at[i], at_line(above))

    def project(s):
        spot = pl.ds(pl.multiple_of(s * per, 16), per)

        @pl.loop(0, groups)
        def _(g):
            cols = pl.ds(pl.multiple_of(g * 2 * gd, 2 * gd), 2 * gd)
            both = jnp.dot(tok_v[s], ug_v[:, cols], preferred_element_type=jnp.float32)
            both = jax.nn.gelu(both.astype(jnp.bfloat16).astype(jnp.float32))
            open_v[g, spot, :] = both[:, :gd]
            act = both[:, gd:]
            act = act - jnp.mean(act, axis=-1, keepdims=True)
            spread = jnp.mean(act * act, axis=-1, keepdims=True)
            norm_v[g, spot, :] = (
                act * lax.rsqrt(spread + norm_eps) * gain_ref[g]
            ).astype(jnp.bfloat16)

        each_z(lambda zz: send_v(zz, s), lambda zz: not inner(zz))

    def out_events(zz, ks):
        for k in ks:
            take_out(zz, k)
            for o in (zz + k, zz - k):
                if 0 <= o < zs:
                    go(plane_first(o))

    if square:
        def in_order(i):
            place = jnp.where(me == sp - 1, 1 - i, i) if i < 2 else i
            return jnp.where((z == 0) | (z == zs - 1), source(place), i)

        for r in range(sp):
            turn = in_order(r)
            for h in range(2):
                @pl.when((turn > 0) & (turn != 1 + h))
                def _():
                    arrived(tok_half(source(turn), h), tok_r.at[turn, h])
            project(source(turn))
            if r == 1 and held_back < groups:
                each_z(lambda zz: own_mix(zz, "dn", held_back, groups), lambda zz: zz == zs - 1)
            if r == sp - 1:
                for q in range(sp // 2, sp):
                    each_z(lambda zz: go(v_copies(zz, q)[1:]), split)

            def events(zz, r=r):
                first = r + 1 if inner(zz) else r
                ks = range(first, zs if r == sp - 1 else first + 1)
                out_events(zz, [k for k in ks if 0 < k < zs])

            each_z(events)
    else:
        @pl.loop(0, sp)
        def _(r):
            @pl.when(r > 0)
            def _():
                for h in range(2):
                    arrived(tok_half(source(r), h), tok_r.at[r, h])

            project(source(r))

        each_z(lambda zz: out_events(zz, range(1, zs)), lambda zz: not inner(zz))

    def take_mix(zz, cc, g, o, onward=True):
        d = o * CORES + cc
        arrived(mx_bytes(d), mx_line.at[g, o])
        if onward:
            go(mx_copies(zz, cc, g, o, "dn" if o > zz else "up"))
        go(mx_copies(zz, cc, g, o, "pair"))

    def passed_on(zz, o):
        return abs(o - zz) == 1 and inner(zz - 1 if o > zz else zz + 1)

    def late(zz, o):
        return zz == zs - 2 and o == zs - 1

    def near_mix(zz, cc):
        for o in (zz + 1, zz - 1):
            if passed_on(zz, o):
                @pl.loop(0, held_back if late(zz, o) else groups)
                def _(g):
                    take_mix(zz, cc, g, o)

    def late_mix(zz, cc):
        @pl.loop(held_back, groups)
        def _(g):
            take_mix(zz, cc, g, zz + 1, not far)

    each_d(near_mix, inner)
    if far:
        each_z(lambda zz: far_send(0, norm_v).start(), lambda zz: zz == below)

    def ready_at(q):
        if block % per:
            return zs - 1
        return (((q + 1) * per - 1) % block) // zr

    def needs(o):
        return min(block, up_to((o + 1) * zr, LANES))

    def first_need(zz, q):
        if not v_useful(mate(zz), q):
            return None
        return next(o for o in range(zs) if o != mate(zz) and (block % per or starts(q) < (o + 1) * zr))

    def with_mate(zz, o):
        return inner(zz) and mate(zz) is not None and mate(zz) != o

    def alone(zz, o):
        return zz == o if not inner(zz) else not with_mate(zz, o)

    def gated_copy(g, q):
        return remote(gated_v.at[g, pl.ds(q * per, per), :], held_v.at[me, g],
                      ga_s.at[0], ga_r.at[g, me], {"sp": q})

    def ret_copy(zz, g, o):
        spot = mixed_v.at[g, :, o]
        return remote(spot, spot, ret_s.at[0], ret_r.at[g, o], at_line(mate(zz)))

    def hand_over(g, o):
        for q in range(sp):
            if ready_at(q) == o:
                @pl.when(me == q)
                def _():
                    held_v[q, g] = gated_v[g, pl.ds(q * per, per), :]

                @pl.when(me != q)
                def _():
                    gated_copy(g, q).start()

    def one_of(zs_in):
        return functools.reduce(jnp.logical_or, [z == zz for zz in zs_in])

    def unit(o, low=0, high=groups, only=None, but=()):
        lo = o * zr
        base, top = lo // LANES * LANES, needs(o)

        def wait_v(zz):
            apart = split(mate(zz))
            for q in range(sp):
                if first_need(zz, q) == o:
                    rows_of = pl.ds(q * per, per)
                    main = pl.ds(0, last_g if apart else groups)
                    arrived(other_v.at[main, rows_of, :], v_r.at[0, q])
                    if apart and o < above:
                        arrived(other_v.at[pl.ds(last_g, 1), rows_of, :], v_r.at[1, q])

        if low == 0:
            each_z(wait_v, lambda zz: with_mate(zz, o) and zz not in but and only in (None, zz))

        def mix(members, paired):
            def rows_from_line(zz, cc):
                @pl.loop(low, high)
                def _(g):
                    take_mix(zz, cc, g, o)

            each_d(rows_from_line, lambda zz: zz in members and o != zz and not passed_on(zz, o))

            @pl.loop(low, high)
            def _(g):
                def rows_in(zz, cc):
                    if not (far and zz == above and o >= above and low == last_g):
                        arrived(mx_bytes(o * CORES + 1 - cc), mx_pr.at[g, o])

                def values(at, end, spare=0):
                    own = norm_v[g, at:end, :]
                    if not paired:
                        return own
                    other = other_v[g, at:end - spare, :]
                    if spare:
                        zeros = jnp.zeros((spare, gd), jnp.bfloat16)
                        other = jnp.concatenate([other, zeros], axis=0)
                    return jnp.concatenate([own, other], axis=1)

                each_d(rows_in, lambda zz: zz in members)
                corner = mix_v[g, o * CORES:(o + 1) * CORES, :, base:top].reshape(zr, top - base)
                keep = lax.broadcasted_iota(jnp.int32, corner.shape, 0) + (lo - base) >= (
                    lax.broadcasted_iota(jnp.int32, corner.shape, 1))
                corner = jnp.where(keep, corner.astype(jnp.float32), 0.0).astype(jnp.bfloat16)
                bias = bias_v[g, lo:lo + zr, :]
                for b in range(blocks):
                    at = b * block
                    mixed = jnp.dot(corner, values(at + base, at + top, top - lo - zr),
                                    preferred_element_type=jnp.float32)
                    if base > 0:
                        left = mix_v[g, o * CORES:(o + 1) * CORES, :, :base].reshape(zr, base)
                        mixed += jnp.dot(left, values(at, at + base),
                                         preferred_element_type=jnp.float32)
                    spot = slice(at + lo, at + lo + zr)
                    if paired:
                        mixed_v[g, b, o] = (mixed[:, gd:] + bias).astype(jnp.bfloat16)
                    gated_v[g, spot, :] = (
                        open_v[g, spot, :] * (mixed[:, :gd] + bias)).astype(jnp.bfloat16)
                if paired:
                    each_z(lambda zz: ret_copy(zz, g, o).start(), lambda zz: zz in members)
                hand_over(g, o)

        for paired, test in ((True, with_mate), (False, alone)):
            members = [zz for zz in range(zs) if test(zz, o) and zz not in but and only in (None, zz)]
            if members:
                pl.when(one_of(members))(functools.partial(mix, members, paired))

        if only is not None:
            return

        waiting = [zz for zz in (0, zs - 1) if zz != o and zz not in but]
        if not waiting:
            return

        @pl.when(one_of(waiting))
        def _():
            @pl.loop(low, high)
            def _(g):
                arrived(mixed_v.at[g, :, o], ret_r.at[g, o])
                for b in range(blocks):
                    spot = slice(b * block + lo, b * block + lo + zr)
                    gated_v[g, spot, :] = (
                        open_v[g, spot, :] * mixed_v[g, b, o].astype(jnp.float32)
                    ).astype(jnp.bfloat16)
                hand_over(g, o)

    def plane_round(zz):
        for o in others(zz):
            for r in range(1, sp):
                if not (square and r == 3):
                    arrived(ow_piece(source(r), o, c), pl_r.at[r, o])
            go(plane_second(zz, o))
            for r in range(1, sp):
                if not (square and r == 3):
                    go(plane_pair(r, o))

    def plane_end(zz):
        for o in others(zz):
            for p in range(halves):
                arrived(second_part(source(3), o, p), p2_r.at[o, p])
            go(plane_pair(3, o))

    def far_forward(zz):
        for q in range(sp):
            if first_need(zz, q) >= above:
                arrived(other_v.at[pl.ds(last_g, 1), pl.ds(q * per, per), :], v_r.at[1, q])
        far_send(1, other_v).start()

    def far_unit(i):
        o = above + i
        lo, top = o * zr, needs(o)
        base = lo // LANES * LANES
        rows_of = slice(o * CORES, (o + 1) * CORES)
        corner = mix_v[last_g, rows_of, :, base:top].reshape(zr, top - base)
        keep = lax.broadcasted_iota(jnp.int32, corner.shape, 0) + (lo - base) >= (
            lax.broadcasted_iota(jnp.int32, corner.shape, 1))
        corner = jnp.where(keep, corner.astype(jnp.float32), 0.0).astype(jnp.bfloat16)
        left = mix_v[last_g, rows_of, :, :base].reshape(zr, base)
        bias = bias_v[last_g, lo:lo + zr, :]

        def values(at, end):
            return jnp.concatenate([far_v[0, at:end, :], far_v[1, at:end, :]], axis=1)

        for b in range(blocks):
            at = b * block
            mixed = jnp.dot(left, values(at, at + base), preferred_element_type=jnp.float32)
            mixed += jnp.dot(corner, values(at + base, at + top), preferred_element_type=jnp.float32)
            for n in range(2):
                far_m[n, i, b] = (mixed[:, n * gd:(n + 1) * gd] + bias).astype(jnp.bfloat16)

    def far_back(i):
        spot = far_m.at[:, i]
        return remote(spot, spot, fm_s.at[i], fm_r.at[i], at_line(below))

    def far_above(zz):
        for i in range(2):
            arrived(far_v.at[i], fv_r.at[i])
        for cc in range(CORES):
            @pl.when(c == cc)
            def _():
                for o in (above, zs - 1):
                    arrived(mx_bytes(o * CORES + 1 - cc), mx_pr.at[last_g, o])
        for i in (1, 0):
            far_unit(i)
            far_back(i).start()

    def far_ret(i):
        return remote(far_m.at[1, i], mixed_v.at[last_g, :, above + i],
                      ret_s.at[0], ret_r.at[last_g, above + i], at_line(below - 1))

    def far_below(zz):
        for i in (1, 0):
            o = above + i
            if zz == below:
                arrived(far_m.at[:, i], fm_r.at[i])
                far_ret(i).start()
            else:
                arrived(mixed_v.at[last_g, :, o], ret_r.at[last_g, o])
            for b in range(blocks):
                spot = slice(b * block + o * zr, b * block + (o + 1) * zr)
                mixed = far_m[0, i, b] if zz == below else mixed_v[last_g, b, o]
                gated_v[last_g, spot, :] = (
                    open_v[last_g, spot, :] * mixed.astype(jnp.float32)).astype(jnp.bfloat16)
            hand_over(last_g, o)

    ends, insides = (0, zs - 1), tuple(range(1, zs - 1))
    unit(zs - 1, 0, held_back, only=zs - 2)
    for o in range(zs // 2):
        unit(o, but=ends)
    if far:
        each_z(far_forward, lambda zz: zz == below)
    each_z(plane_round)

    unit(zs - 1, only=zs - 1)
    lower = (below - 1, below)
    for o in range(zs - 1):
        if o < zs // 2:
            unit(o, but=insides)
        elif far and o == above:
            each_d(late_mix, lambda zz: late(zz, zz + 1))
            each_z(far_above, lambda zz: zz == above)
            unit(o, 0, last_g)
            unit(o, last_g, groups, but=lower)
        else:
            unit(o)
    if held_back < groups and not far:
        each_d(late_mix, lambda zz: late(zz, zz + 1))

    def gather_part(g, first):
        for s in range(sp):
            @pl.when(me != s)
            def _():
                arrived(held_v.at[s, g], ga_r.at[g, s])
        squares = jnp.zeros((per, gd), jnp.float32)
        for s in range(sp):
            value = held_v[s, g].astype(jnp.float32)
            squares += value * value
            cols = pl.ds(pl.multiple_of(s * chans + g * gd, LANES), gd)
            normed_v[g, :, s * pk:(s + 1) * pk] = (value * ogain_ref[:, cols]).astype(jnp.bfloat16)
        sums_v[...] = squares if first else sums_v[...] + squares

    step = 4 * ncol if width % (4 * ncol) == 0 else ncol

    def part_dot(p, cols):
        return jnp.dot(normed_v[p], outw_v[p, :, :, cols].reshape(sp * pk, step),
                       preferred_element_type=jnp.float32)

    def weights_here():
        arrived(outw_v.at[:, :, :, own_cols], ow_own.at[1])
        arrived(ow_bytes(zs - 1), ow_pr.at[0])
        for r in range(1, sp):
            arrived(ow_bytes(zs - 1), pp_r.at[r])

    started = []

    def add_parts(which):
        for g in which:
            gather_part(g, not started)
            started.append(g)

        @pl.loop(0, width // step)
        def _(t):
            cols = pl.ds(pl.multiple_of(t * step, LANES), step)
            more = sum(part_dot(p, cols) for p in which)
            part_v[:, cols] = more if len(started) == len(which) else part_v[:, cols] + more

    done = (zs - 1, zs - 2)
    if far:
        unit(zs - 1, 0, last_g - 1, but=done)
        early = (z == 0) & (me < sp // 2)

        def first_parts():
            started.clear()
            weights_here()
            add_parts(range(last_g - 1))

        if square:
            each_z(plane_end)
        pl.when(early)(first_parts)
        each_z(far_below, lambda zz: zz in lower)
        unit(zs - 1, last_g - 1, last_g, but=done)
        unit(zs - 1, last_g, groups, but=lower + (zs - 1,))
        pl.when(jnp.logical_not(early))(first_parts)
        final = jnp.where(me == sp - 1, last_g - 1, last_g)
        add_parts([2 * last_g - 1 - final])
    elif groups > 1:
        if square:
            each_z(plane_end)
        weights_here()
        unit(zs - 1, 0, last_g, but=done)
        add_parts(range(last_g))
        unit(zs - 1, last_g, groups, but=(zs - 1,))
        final = last_g
    else:
        if square:
            each_z(plane_end)
        weights_here()
        unit(zs - 1, but=done)
        final = 0
    gather_part(final, not started)
    scale = lax.rsqrt(jnp.sum(sums_v[...], axis=-1, keepdims=True) / (sp * chans) + norm_eps)

    @pl.loop(0, width // step)
    def _(t):
        cols = pl.ds(pl.multiple_of(t * step, LANES), step)
        last = part_dot(final, cols)
        if started:
            last += part_v[:, cols]
        out_ref[:, cols] = (last * scale).astype(jnp.bfloat16)

    sent(tok_v.at[pl.ds(0, sp - 1)], tok_s.at[0])
    sent(outw_v.at[:, :, :, own_cols], ow_own.at[0])
    for r in range(1, sp):
        if not (square and r == 3):
            sent(ow_bytes(zs - 1), pl_s.at[r])
        sent(ow_bytes(zs - 1), pp_s.at[r])
    if square:
        sent(ow_bytes(zs - 1), p2_s.at[0])
    sent(ow_bytes(zs - 1), ow_send.at[2])
    sent(ug_v.at[pl.ds(0, zs * depth), :], ug_send.at[2])
    sent(held_v.at[pl.ds(0, sp - 1)], ga_s.at[0])

    def line_sent(zz):
        for n, way in ((zz + 1 if zz < zs - 1 else 0, 0), (zs - zz if zz > 0 else 0, 1)):
            if n:
                sent(ug_v.at[pl.ds(0, n * depth), :], ug_send.at[way])
                sent(ow_bytes(n), ow_send.at[way])
        if not inner(zz):
            n = sum(v_useful(zz, q) for q in range(sp))
            main = pl.ds(0, last_g if split(zz) else groups)
            sent(norm_v.at[main, pl.ds(0, n * per), :], v_s.at[0])
            if split(zz):
                sent(norm_v.at[pl.ds(0, 1), pl.ds(0, n * per), :], v_s.at[1])
        elif mate(zz) is not None:
            n = sum(with_mate(zz, o) for o in range(zs))
            sent(mixed_v.at[:, :, pl.ds(0, n)], ret_s.at[0])
        for i in range(2):
            if far and zz == below:
                sent(far_v.at[i], fv_s.at[i])
            if far and zz == above:
                sent(far_m.at[:, i], fm_s.at[i])

    each_z(line_sent)

    def mix_sent(zz, cc):
        for o in range(zs):
            d = o * CORES + cc
            for i, (r0, rn, cols) in enumerate(cuts(d)):
                spot = mix_v.at[:, d, pl.ds(r0, rn), pl.ds(0, cols)]
                if not (inner(zz) or o == zz):
                    continue
                if o >= zz and inner(zz - 1):
                    crossing = last_g if far and zz == above else groups
                    sent(mix_v.at[pl.ds(0, crossing), d, pl.ds(r0, rn), pl.ds(0, cols)],
                         mx_dn.at[o, i])
                if o <= zz and inner(zz + 1):
                    sent(spot, mx_up.at[o, i])
                paired = last_g if far and zz == below and o >= above else groups
                sent(mix_v.at[pl.ds(0, paired), d, pl.ds(r0, rn), pl.ds(0, cols)], mx_ps.at[o, i])

    each_d(mix_sent)


def body(tokens, up_weight, gate_weight, group_gain, mix_weight, mix_bias, out_gain, out_weight):
    per, width = tokens.shape[1:]
    groups, gd = group_gain.shape
    rows, block = mix_weight.shape[1:]
    sp, dps = lax.axis_size("sp"), lax.axis_size("dp")
    zs = dps // CORES
    total = sp * per
    parts = groups
    halves = 1 if parts % 2 else 2
    bf, f32 = jnp.bfloat16, jnp.float32
    dma = pltpu.SemaphoreType.DMA
    hbm = pl.BlockSpec(memory_space=pltpu.HBM)
    vmem = pl.BlockSpec(memory_space=pltpu.VMEM)
    output = pl.pallas_call(
        functools.partial(fused_kernel, sp, zs),
        out_shape=pltpu.VMEM((per, width), bf),
        in_specs=[hbm, hbm, hbm, vmem, hbm, vmem, vmem, hbm],
        out_specs=vmem,
        scratch_shapes=[
            pltpu.VMEM((sp, per, width), bf),
            pltpu.VMEM((width, 2 * groups * gd), bf),
            pltpu.VMEM((groups, dps, rows, block), bf),
            pltpu.VMEM((parts, sp, groups * gd // parts, width), bf),
            pltpu.VMEM((groups, total, gd), f32),
            pltpu.VMEM((groups, total, gd), bf),
            pltpu.VMEM((groups, total, gd), bf),
            pltpu.VMEM((groups, block, gd), f32),
            pltpu.VMEM((groups, total // block, zs, CORES * rows, gd), bf),
            pltpu.VMEM((groups, total, gd), bf),
            pltpu.VMEM((sp, groups, per, gd), bf),
            pltpu.VMEM((parts, per, sp * groups * gd // parts), bf),
            pltpu.VMEM((per, gd), f32),
            pltpu.VMEM((per, width if parts > 1 else gd), f32),
            pltpu.VMEM((2, total if parts > 2 else 16, gd), bf),
            pltpu.VMEM((2, 2, total // block, CORES * rows if parts > 2 else 16, gd), bf),
            dma((4,)),
            dma((zs, 2)), dma((3,)), dma((1,)),
            dma((zs,)), dma((3,)), dma((1,)), dma((2,)),
            dma((sp,)), dma((sp, zs)), dma((1,)), dma((zs, halves)), dma((sp,)), dma((sp,)),
            dma((groups, zs)), dma((groups, zs)), dma((zs, 2)), dma((zs, 2)), dma((zs, 2)),
            dma((1,)), dma((sp, 2)), dma((2,)), dma((2, sp)),
            dma((1,)), dma((groups, zs)), dma((1,)), dma((parts, sp)),
            dma((2,)), dma((2,)), dma((2,)), dma((2,)),
        ],
        compiler_params=pltpu.CompilerParams(collective_id=0, has_side_effects=True, vmem_limit_bytes=65_000_000),
    )(tokens.reshape(per, width), up_weight, gate_weight, group_gain[:, None, :], mix_weight, mix_bias,
      out_gain[None, :], out_weight.reshape(sp, parts, groups * gd // parts, -1))
    return output.reshape(tokens.shape)


def solution(mesh):
    return jax.shard_map(
        body,
        mesh=mesh,
        in_specs=(
            P("dp", "sp", None),
            P("dp", None),
            P("dp", None),
            P("sp", None),
            P("sp", "dp", None),
            P("sp", None),
            P(),
            P(None, "dp"),
        ),
        out_specs=P("dp", "sp", None),
        check_vma=False,
    )
```

```python
import functools

import jax
import jax.numpy as jnp
from jax import lax
from jax.experimental import pallas as pl
from jax.experimental.pallas import tpu as pltpu
from jax.sharding import PartitionSpec as P

norm_eps = 1e-06
CORES = 2
LANES = 128
MESH = pl.DeviceIdType.MESH


def up_to(n, m):
    return -(-n // m) * m


def fused_kernel(
    sp, zs,
    tok_ref, up_ref, gate_ref, gain_ref, mix_ref, bias_ref, ogain_ref, outw_ref, out_ref,
    tok_v, ug_v, mix_v, outw_v, open_v, norm_v, other_v, bias_v, mixed_v, gated_v, held_v,
    normed_v, sums_v, part_v, far_v, far_m,
    load_sem, ug_line, ug_send, ug_pr, ow_line, ow_send, ow_pr, ow_own,
    pl_s, pl_r, p2_s, p2_r, pp_s, pp_r, mx_line, mx_pr, mx_up, mx_dn, mx_ps,
    tok_s, tok_r, v_s, v_r, ret_s, ret_r, ga_s, ga_r, fv_s, fv_r, fm_s, fm_r,
):
    me = lax.axis_index("sp")
    dp = lax.axis_index("dp")
    z, c = dp // CORES, lax.rem(dp, CORES)
    groups, dps, rows, block = mix_v.shape
    per, width = out_ref.shape
    gd = gain_ref.shape[2]
    chans = groups * gd
    depth, ncol = up_ref.shape[0], outw_ref.shape[3]
    total = sp * per
    blocks = total // block
    parts, _, pk, _ = outw_v.shape
    halves = 1 if parts % 2 else 2
    hp = parts // halves
    zr = CORES * rows
    half, dhalf = per // 2, depth // 2
    square = sp == 4
    far = zs == 4 and groups > 2
    below, above, last_g = zs // 2 - 1, zs // 2, groups - 1

    partner = {"dp": z * CORES + (1 - c)}

    def at_line(zz):
        return {"dp": zz * CORES + c}

    def around(r, sign):
        if square:
            y = lax.rem(me // 2 + r // 2, 2)
            x = lax.rem(lax.rem(me, 2) + r % 2, 2)
            return y * 2 + x
        return lax.rem(me + sign * r + sp, sp)

    def target(r):
        return around(r, 1)

    def source(r):
        return around(r, -1)

    def peer(r):
        return {"sp": target(r)}

    def inner(zz):
        return 0 < zz < zs - 1

    def mate(zz):
        return {0: 1, 1: 0, zs - 1: zs - 2, zs - 2: zs - 1}.get(zz)

    def remote(src, dst, send, recv, device):
        return pltpu.make_async_remote_copy(
            src_ref=src, dst_ref=dst, send_sem=send, recv_sem=recv,
            device_id=device, device_id_type=MESH)

    def sent(ref, sem):
        remote(ref, ref, sem, sem, partner).wait_send()

    def arrived(ref, sem):
        remote(ref, ref, sem, sem, partner).wait_recv()

    def each_z(fn, only=None):
        for zz in range(zs):
            if only is None or only(zz):
                pl.when(z == zz)(functools.partial(fn, zz))

    def each_d(fn, only=None):
        for zz in range(zs):
            if only is None or only(zz):
                for cc in range(CORES):
                    pl.when(dp == zz * CORES + cc)(functools.partial(fn, zz, cc))

    loads = {"ug": [], "tok": [], "ow": [], "mx": []}
    for g in range(groups):
        for t, ref in enumerate((up_ref, gate_ref)):
            cols = pl.ds(pl.multiple_of(me * chans + g * gd, LANES), gd)
            spot = 2 * g + t
            loads["ug"].append(pltpu.make_async_copy(
                ref.at[:, cols],
                ug_v.at[pl.ds(dp * depth, depth), pl.ds(spot * gd, gd)],
                load_sem.at[3]))
    loads["tok"].append(pltpu.make_async_copy(tok_ref, tok_v.at[me], load_sem.at[0]))
    own_cols = pl.ds(pl.multiple_of(dp * ncol, LANES), ncol)
    for p in range(parts):
        loads["ow"].append(pltpu.make_async_copy(
            outw_ref.at[:, p], outw_v.at[p, :, :, own_cols], load_sem.at[1]))
    loads["mx"].append(pltpu.make_async_copy(mix_ref, mix_v.at[:, dp], load_sem.at[2]))
    for kind in ("ug", "tok", "ow", "mx"):
        for load in loads[kind]:
            load.start()

    def loaded(ref, sem):
        pltpu.make_async_copy(ref, ref, sem).wait()

    barrier = pltpu.get_barrier_semaphore()

    def greet(zz):
        friends = [partner] + [peer(r) for r in range(1, sp)]
        if zz > 0:
            friends.append(at_line(zz - 1))
        if zz < zs - 1:
            friends.append(at_line(zz + 1))
        for friend in friends:
            pl.semaphore_signal(barrier, inc=1, device_id=friend, device_id_type=MESH)
        pl.semaphore_wait(barrier, len(friends))

    each_z(greet)

    def ug_piece(o, cc, h):
        return ug_v.at[pl.ds((o * CORES + cc) * depth + h * dhalf, dhalf), :]

    def ow_piece(s, o, cc):
        cols = pl.ds(pl.multiple_of((o * CORES + cc) * ncol, LANES), ncol)
        return outw_v.at[:, s, :, cols]

    def cuts(d):
        out, at, end = [], d * rows, (d + 1) * rows
        while at < end:
            top = min(end, (at // LANES + 1) * LANES)
            out.append((at - d * rows, top - at, min(block, up_to(top, LANES))))
            at = top
        return out

    def mx_bytes(d):
        size = sum(rn * cols for _, rn, cols in cuts(d))
        return open_v.at[0, pl.ds(0, size // gd // 2), :]

    def mx_piece(g, d, piece):
        r0, rn, cols = piece
        return mix_v.at[g, d, pl.ds(r0, rn), pl.ds(0, cols)]

    def ug_copies(zz, o, h):
        src, out = ug_piece(o, c, h), []
        if o >= zz and zz > 0:
            out.append(remote(src, src, ug_send.at[1], ug_line.at[o, h], at_line(zz - 1)))
        if o <= zz and zz < zs - 1:
            out.append(remote(src, src, ug_send.at[0], ug_line.at[o, h], at_line(zz + 1)))
        out.append(remote(src, src, ug_send.at[2], ug_pr.at[0], partner))
        return out

    def ow_down(zz, o):
        src = ow_piece(me, o, c)
        if o >= zz and zz > 0:
            return [remote(src, src, ow_send.at[1], ow_line.at[o], at_line(zz - 1))]
        return []

    def ow_rise(zz, o):
        src = ow_piece(me, o, c)
        if o <= zz and zz < zs - 1:
            return [remote(src, src, ow_send.at[0], ow_line.at[o], at_line(zz + 1))]
        return []

    def ow_pair(o):
        src = ow_piece(me, o, c)
        return [remote(src, src, ow_send.at[2], ow_pr.at[0], partner)]

    def ow_own_pair():
        src = outw_v.at[:, :, :, own_cols]
        return [remote(src, src, ow_own.at[0], ow_own.at[1], partner)]

    def ow_bytes(n):
        return outw_v.at[:, 0, :, pl.ds(0, n * ncol)]

    def mx_copies(zz, cc, g, o, way):
        out = []
        d = o * CORES + cc
        for i, piece in enumerate(cuts(d)):
            src = mx_piece(g, d, piece)
            if way == "dn" and o >= zz and inner(zz - 1):
                out.append(remote(src, src, mx_dn.at[o, i], mx_line.at[g, o], at_line(zz - 1)))
            if way == "up" and o <= zz and inner(zz + 1):
                out.append(remote(src, src, mx_up.at[o, i], mx_line.at[g, o], at_line(zz + 1)))
            if way == "pair" and (inner(zz) or o == zz):
                out.append(remote(src, src, mx_ps.at[o, i], mx_pr.at[g, o], partner))
        return out

    def go(copies):
        for copy in copies:
            copy.start()

    def own_mix(zz, way, low=0, high=groups):
        if far and zz == above and way == "dn":
            high = min(high, last_g)

        for cc in range(CORES):
            @pl.when(c == cc)
            def _():
                @pl.loop(low, high)
                def _(g):
                    go(mx_copies(zz, cc, g, zz, way))

    def ug_left(zz, way, k):
        far = zs - 1 - zz if way == "dn" else zz
        there = zz > 0 if way == "dn" else zz < zs - 1
        return there, max(0, far - k)

    held_back = max(1, groups - 1)

    def own_out(zz, way):
        go(ow_down(zz, zz) if way == "dn" else ow_rise(zz, zz))

    loaded(ug_v.at[pl.ds(dp * depth, depth), :], load_sem.at[3])

    def first_weights(zz):
        for h in range(2):
            go(ug_copies(zz, zz, h))

    each_z(first_weights)
    for load in loads["tok"]:
        load.wait()

    def tok_half(s, h):
        return tok_v.at[s, pl.ds(h * half, half), :]

    def tok_copy(s, r, h, r_there):
        return remote(tok_half(s, h), tok_half(s, h), tok_s.at[0], tok_r.at[r_there, h], peer(r))

    def tok_first():
        if square:
            return [tok_copy(me, 1, 0, 1), tok_copy(me, 2, 1, 2), tok_copy(me, 1, 1, 1), tok_copy(me, 2, 0, 2)]
        return [tok_copy(me, r, h, r) for r in range(1, sp) for h in range(2)]

    def tok_second():
        if square:
            return [tok_copy(source(1), 2, 0, 3), tok_copy(source(2), 1, 1, 3)]
        return []

    go(tok_first())
    loaded(outw_v.at[:, :, :, own_cols], load_sem.at[1])
    loads["mx"][0].wait()
    go(ow_own_pair())

    def first_rest(zz):
        for way in ("dn", "up"):
            there, left = ug_left(zz, way, 0)
            if there and left == 0:
                own_out(zz, way)
                own_mix(zz, way, 0, held_back if zz == zs - 1 else groups)
        own_mix(zz, "pair")

    each_z(first_rest)

    for g in range(groups):
        for t in range(block // LANES):
            spot = slice(t * LANES, (t + 1) * LANES)
            bias_v[g, spot, :] = jnp.broadcast_to(bias_ref[g:g + 1, spot], (gd, LANES)).T

    def take_ug(zz, k):
        for o in (zz + k, zz - k):
            if 0 <= o < zs:
                for h in range(2):
                    arrived(ug_piece(o, c, h), ug_line.at[o, h])
                    go(ug_copies(zz, o, h))
        for way in ("dn", "up"):
            there, left = ug_left(zz, way, k)
            before = ug_left(zz, way, k - 1)[1]
            if there and left == 0 and before > 0:
                own_out(zz, way)
                own_mix(zz, way, 0, 1)

    def take_out(zz, k):
        for o in (zz + k, zz - k):
            if 0 <= o < zs:
                arrived(ow_piece(me, o, c), ow_line.at[o])
                go(ow_down(zz, o) if o > zz else ow_rise(zz, o))
                go(ow_pair(o))
        for way in ("dn", "up"):
            there, left = ug_left(zz, way, k)
            before = ug_left(zz, way, k - 1)[1]
            if there and left == 0 and before > 0:
                own_mix(zz, way, 1, groups)

    def others(zz):
        return [o for k in range(1, zs) for o in (zz + k, zz - k) if 0 <= o < zs]

    def plane_first(o):
        src = ow_piece(me, o, c)
        reach = (1, 2) if square else range(1, sp)
        return [remote(src, src, pl_s.at[r], pl_r.at[r, o], peer(r)) for r in reach]

    def second_part(s, o, p):
        cols = pl.ds(pl.multiple_of((o * CORES + c) * ncol, LANES), ncol)
        return outw_v.at[pl.ds(p * hp, hp), s, :, cols]

    def plane_second(zz, o):
        if not square:
            return []
        units = [(x, p) for x in others(zz) for p in range(halves)]
        out = []
        for p in range(halves):
            via, to = (1, 2) if units.index((o, p)) < len(units) // 2 else (2, 1)
            src = second_part(source(via), o, p)
            out.append(remote(src, src, p2_s.at[0], p2_r.at[o, p], peer(to)))
        return out

    def plane_pair(r, o):
        src = ow_piece(source(r), o, c)
        return [remote(src, src, pp_s.at[r], pp_r.at[r], partner)]

    each_z(lambda zz: take_ug(zz, 1))
    if square:
        arrived(tok_half(source(1), 0), tok_r.at[1, 0])
        arrived(tok_half(source(2), 1), tok_r.at[2, 1])
    go(tok_second())

    def more_weights(zz):
        for k in range(2, zs):
            take_ug(zz, k)
        if inner(zz) and not square:
            for k in range(1, zs):
                take_out(zz, k)
            for o in others(zz):
                go(plane_first(o))

    each_z(more_weights)

    arrived(ug_v.at[pl.ds(0, zs * depth), :], ug_pr.at[0])

    def split(zz):
        return far and zz == below - 1

    def v_copies(zz, q):
        spot = pl.ds(pl.multiple_of(q * per, 16), per)
        ranges = ((last_g, 1), (0, last_g)) if split(zz) else ((0, groups),)
        out = []
        for i, (g0, gn) in enumerate(ranges):
            which = len(ranges) - 1 - i
            src, dst = (ref.at[pl.ds(g0, gn), spot, :] for ref in (norm_v, other_v))
            out.append(remote(src, dst, v_s.at[which], v_r.at[which, q], at_line(mate(zz))))
        return out

    def starts(q):
        return (q * per) % block

    def v_useful(end, q):
        return any(starts(q) < (o + 1) * zr for o in range(zs) if o != end) or block % per > 0

    def send_v(zz, s):
        for q in range(sp):
            if v_useful(zz, q):
                late_main = split(zz) and q >= sp // 2
                pl.when(s == q)(lambda q=q, n=1 if late_main else 2: go(v_copies(zz, q)[:n]))

    def far_send(i, ref):
        return remote(ref.at[last_g], far_v.at[i], fv_s.at[i], fv_r.at[i], at_line(above))

    def project(s):
        spot = pl.ds(pl.multiple_of(s * per, 16), per)

        @pl.loop(0, groups)
        def _(g):
            cols = pl.ds(pl.multiple_of(g * 2 * gd, 2 * gd), 2 * gd)
            both = jnp.dot(tok_v[s], ug_v[:, cols], preferred_element_type=jnp.float32)
            both = jax.nn.gelu(both.astype(jnp.bfloat16).astype(jnp.float32))
            open_v[g, spot, :] = both[:, :gd]
            act = both[:, gd:]
            act = act - jnp.mean(act, axis=-1, keepdims=True)
            spread = jnp.mean(act * act, axis=-1, keepdims=True)
            norm_v[g, spot, :] = (
                act * lax.rsqrt(spread + norm_eps) * gain_ref[g]
            ).astype(jnp.bfloat16)

        each_z(lambda zz: send_v(zz, s), lambda zz: not inner(zz))

    def out_events(zz, ks):
        for k in ks:
            take_out(zz, k)
            for o in (zz + k, zz - k):
                if 0 <= o < zs:
                    go(plane_first(o))

    if square:
        def in_order(i):
            place = jnp.where(me == sp - 1, 1 - i, i) if i < 2 else i
            return jnp.where((z == 0) | (z == zs - 1), source(place), i)

        for r in range(sp):
            turn = in_order(r)
            for h in range(2):
                @pl.when((turn > 0) & (turn != 1 + h))
                def _():
                    arrived(tok_half(source(turn), h), tok_r.at[turn, h])
            project(source(turn))
            if r == 1 and held_back < groups:
                each_z(lambda zz: own_mix(zz, "dn", held_back, groups), lambda zz: zz == zs - 1)
            if r == sp - 1:
                for q in range(sp // 2, sp):
                    each_z(lambda zz: go(v_copies(zz, q)[1:]), split)

            def events(zz, r=r):
                first = r + 1 if inner(zz) else r
                ks = range(first, zs if r == sp - 1 else first + 1)
                out_events(zz, [k for k in ks if 0 < k < zs])

            each_z(events)
    else:
        @pl.loop(0, sp)
        def _(r):
            @pl.when(r > 0)
            def _():
                for h in range(2):
                    arrived(tok_half(source(r), h), tok_r.at[r, h])

            project(source(r))

        each_z(lambda zz: out_events(zz, range(1, zs)), lambda zz: not inner(zz))

    def take_mix(zz, cc, g, o, onward=True):
        d = o * CORES + cc
        arrived(mx_bytes(d), mx_line.at[g, o])
        if onward:
            go(mx_copies(zz, cc, g, o, "dn" if o > zz else "up"))
        go(mx_copies(zz, cc, g, o, "pair"))

    def passed_on(zz, o):
        return abs(o - zz) == 1 and inner(zz - 1 if o > zz else zz + 1)

    def late(zz, o):
        return zz == zs - 2 and o == zs - 1

    def near_mix(zz, cc):
        for o in (zz + 1, zz - 1):
            if passed_on(zz, o):
                @pl.loop(0, held_back if late(zz, o) else groups)
                def _(g):
                    take_mix(zz, cc, g, o)

    def late_mix(zz, cc):
        @pl.loop(held_back, groups)
        def _(g):
            take_mix(zz, cc, g, zz + 1, not far)

    each_d(near_mix, inner)
    if far:
        each_z(lambda zz: far_send(0, norm_v).start(), lambda zz: zz == below)

    def ready_at(q):
        if block % per:
            return zs - 1
        return (((q + 1) * per - 1) % block) // zr

    def needs(o):
        return min(block, up_to((o + 1) * zr, LANES))

    def first_need(zz, q):
        if not v_useful(mate(zz), q):
            return None
        return next(o for o in range(zs) if o != mate(zz) and (block % per or starts(q) < (o + 1) * zr))

    def with_mate(zz, o):
        return inner(zz) and mate(zz) is not None and mate(zz) != o

    def alone(zz, o):
        return zz == o if not inner(zz) else not with_mate(zz, o)

    def gated_copy(g, q):
        return remote(gated_v.at[g, pl.ds(q * per, per), :], held_v.at[me, g],
                      ga_s.at[0], ga_r.at[g, me], {"sp": q})

    def ret_copy(zz, g, o):
        spot = mixed_v.at[g, :, o]
        return remote(spot, spot, ret_s.at[0], ret_r.at[g, o], at_line(mate(zz)))

    def hand_over(g, o):
        for q in range(sp):
            if ready_at(q) == o:
                @pl.when(me == q)
                def _():
                    held_v[q, g] = gated_v[g, pl.ds(q * per, per), :]

                @pl.when(me != q)
                def _():
                    gated_copy(g, q).start()

    def one_of(zs_in):
        return functools.reduce(jnp.logical_or, [z == zz for zz in zs_in])

    def unit(o, low=0, high=groups, only=None, but=()):
        lo = o * zr
        base, top = lo // LANES * LANES, needs(o)

        def wait_v(zz):
            apart = split(mate(zz))
            for q in range(sp):
                if first_need(zz, q) == o:
                    rows_of = pl.ds(q * per, per)
                    main = pl.ds(0, last_g if apart else groups)
                    arrived(other_v.at[main, rows_of, :], v_r.at[0, q])
                    if apart and o < above:
                        arrived(other_v.at[pl.ds(last_g, 1), rows_of, :], v_r.at[1, q])

        if low == 0:
            each_z(wait_v, lambda zz: with_mate(zz, o) and zz not in but and only in (None, zz))

        def mix(members, paired):
            def rows_from_line(zz, cc):
                @pl.loop(low, high)
                def _(g):
                    take_mix(zz, cc, g, o)

            each_d(rows_from_line, lambda zz: zz in members and o != zz and not passed_on(zz, o))

            @pl.loop(low, high)
            def _(g):
                def rows_in(zz, cc):
                    if not (far and zz == above and o >= above and low == last_g):
                        arrived(mx_bytes(o * CORES + 1 - cc), mx_pr.at[g, o])

                def values(at, end, spare=0):
                    own = norm_v[g, at:end, :]
                    if not paired:
                        return own
                    other = other_v[g, at:end - spare, :]
                    if spare:
                        zeros = jnp.zeros((spare, gd), jnp.bfloat16)
                        other = jnp.concatenate([other, zeros], axis=0)
                    return jnp.concatenate([own, other], axis=1)

                each_d(rows_in, lambda zz: zz in members)
                corner = mix_v[g, o * CORES:(o + 1) * CORES, :, base:top].reshape(zr, top - base)
                keep = lax.broadcasted_iota(jnp.int32, corner.shape, 0) + (lo - base) >= (
                    lax.broadcasted_iota(jnp.int32, corner.shape, 1))
                corner = jnp.where(keep, corner.astype(jnp.float32), 0.0).astype(jnp.bfloat16)
                bias = bias_v[g, lo:lo + zr, :]
                for b in range(blocks):
                    at = b * block
                    mixed = jnp.dot(corner, values(at + base, at + top, top - lo - zr),
                                    preferred_element_type=jnp.float32)
                    if base > 0:
                        left = mix_v[g, o * CORES:(o + 1) * CORES, :, :base].reshape(zr, base)
                        mixed += jnp.dot(left, values(at, at + base),
                                         preferred_element_type=jnp.float32)
                    spot = slice(at + lo, at + lo + zr)
                    if paired:
                        mixed_v[g, b, o] = (mixed[:, gd:] + bias).astype(jnp.bfloat16)
                    gated_v[g, spot, :] = (
                        open_v[g, spot, :] * (mixed[:, :gd] + bias)).astype(jnp.bfloat16)
                if paired:
                    each_z(lambda zz: ret_copy(zz, g, o).start(), lambda zz: zz in members)
                hand_over(g, o)

        for paired, test in ((True, with_mate), (False, alone)):
            members = [zz for zz in range(zs) if test(zz, o) and zz not in but and only in (None, zz)]
            if members:
                pl.when(one_of(members))(functools.partial(mix, members, paired))

        if only is not None:
            return

        waiting = [zz for zz in (0, zs - 1) if zz != o and zz not in but]
        if not waiting:
            return

        @pl.when(one_of(waiting))
        def _():
            @pl.loop(low, high)
            def _(g):
                arrived(mixed_v.at[g, :, o], ret_r.at[g, o])
                for b in range(blocks):
                    spot = slice(b * block + lo, b * block + lo + zr)
                    gated_v[g, spot, :] = (
                        open_v[g, spot, :] * mixed_v[g, b, o].astype(jnp.float32)
                    ).astype(jnp.bfloat16)
                hand_over(g, o)

    def plane_round(zz):
        for o in others(zz):
            for r in range(1, sp):
                if not (square and r == 3):
                    arrived(ow_piece(source(r), o, c), pl_r.at[r, o])
            go(plane_second(zz, o))
            for r in range(1, sp):
                if not (square and r == 3):
                    go(plane_pair(r, o))

    def plane_end(zz):
        for o in others(zz):
            for p in range(halves):
                arrived(second_part(source(3), o, p), p2_r.at[o, p])
            go(plane_pair(3, o))

    def far_forward(zz):
        for q in range(sp):
            if first_need(zz, q) >= above:
                arrived(other_v.at[pl.ds(last_g, 1), pl.ds(q * per, per), :], v_r.at[1, q])
        far_send(1, other_v).start()

    def far_unit(i):
        o = above + i
        lo, top = o * zr, needs(o)
        base = lo // LANES * LANES
        rows_of = slice(o * CORES, (o + 1) * CORES)
        corner = mix_v[last_g, rows_of, :, base:top].reshape(zr, top - base)
        keep = lax.broadcasted_iota(jnp.int32, corner.shape, 0) + (lo - base) >= (
            lax.broadcasted_iota(jnp.int32, corner.shape, 1))
        corner = jnp.where(keep, corner.astype(jnp.float32), 0.0).astype(jnp.bfloat16)
        left = mix_v[last_g, rows_of, :, :base].reshape(zr, base)
        bias = bias_v[last_g, lo:lo + zr, :]

        def values(at, end):
            return jnp.concatenate([far_v[0, at:end, :], far_v[1, at:end, :]], axis=1)

        for b in range(blocks):
            at = b * block
            mixed = jnp.dot(left, values(at, at + base), preferred_element_type=jnp.float32)
            mixed += jnp.dot(corner, values(at + base, at + top), preferred_element_type=jnp.float32)
            for n in range(2):
                far_m[n, i, b] = (mixed[:, n * gd:(n + 1) * gd] + bias).astype(jnp.bfloat16)

    def far_back(i):
        spot = far_m.at[:, i]
        return remote(spot, spot, fm_s.at[i], fm_r.at[i], at_line(below))

    def far_above(zz):
        for i in range(2):
            arrived(far_v.at[i], fv_r.at[i])
        for cc in range(CORES):
            @pl.when(c == cc)
            def _():
                for o in (above, zs - 1):
                    arrived(mx_bytes(o * CORES + 1 - cc), mx_pr.at[last_g, o])
        for i in (1, 0):
            far_unit(i)
            far_back(i).start()

    def far_ret(i):
        return remote(far_m.at[1, i], mixed_v.at[last_g, :, above + i],
                      ret_s.at[0], ret_r.at[last_g, above + i], at_line(below - 1))

    def far_below(zz):
        for i in (1, 0):
            o = above + i
            if zz == below:
                arrived(far_m.at[:, i], fm_r.at[i])
                far_ret(i).start()
            else:
                arrived(mixed_v.at[last_g, :, o], ret_r.at[last_g, o])
            for b in range(blocks):
                spot = slice(b * block + o * zr, b * block + (o + 1) * zr)
                mixed = far_m[0, i, b] if zz == below else mixed_v[last_g, b, o]
                gated_v[last_g, spot, :] = (
                    open_v[last_g, spot, :] * mixed.astype(jnp.float32)).astype(jnp.bfloat16)
            hand_over(last_g, o)

    ends, insides = (0, zs - 1), tuple(range(1, zs - 1))
    unit(zs - 1, 0, held_back, only=zs - 2)
    for o in range(zs // 2):
        unit(o, but=ends)
    if far:
        each_z(far_forward, lambda zz: zz == below)
    each_z(plane_round)

    unit(zs - 1, only=zs - 1)
    lower = (below - 1, below)
    for o in range(zs - 1):
        if o < zs // 2:
            unit(o, but=insides)
        elif far and o == above:
            each_d(late_mix, lambda zz: late(zz, zz + 1))
            each_z(far_above, lambda zz: zz == above)
            unit(o, 0, last_g)
            unit(o, last_g, groups, but=lower)
        else:
            unit(o)
    if held_back < groups and not far:
        each_d(late_mix, lambda zz: late(zz, zz + 1))

    def gather_part(g, first):
        for s in range(sp):
            @pl.when(me != s)
            def _():
                arrived(held_v.at[s, g], ga_r.at[g, s])
        squares = jnp.zeros((per, gd), jnp.float32)
        for s in range(sp):
            value = held_v[s, g].astype(jnp.float32)
            squares += value * value
            cols = pl.ds(pl.multiple_of(s * chans + g * gd, LANES), gd)
            normed_v[g, :, s * pk:(s + 1) * pk] = (value * ogain_ref[:, cols]).astype(jnp.bfloat16)
        sums_v[...] = squares if first else sums_v[...] + squares

    step = 8 * ncol if width % (8 * ncol) == 0 else ncol

    def part_dot(p, cols):
        return jnp.dot(normed_v[p], outw_v[p, :, :, cols].reshape(sp * pk, step),
                       preferred_element_type=jnp.float32)

    def weights_here():
        arrived(outw_v.at[:, :, :, own_cols], ow_own.at[1])
        arrived(ow_bytes(zs - 1), ow_pr.at[0])
        for r in range(1, sp):
            arrived(ow_bytes(zs - 1), pp_r.at[r])

    started = []

    def add_parts(which):
        for g in which:
            gather_part(g, not started)
            started.append(g)

        @pl.loop(0, width // step)
        def _(t):
            cols = pl.ds(pl.multiple_of(t * step, LANES), step)
            more = sum(part_dot(p, cols) for p in which)
            part_v[:, cols] = more if len(started) == len(which) else part_v[:, cols] + more

    done = (zs - 1, zs - 2)
    if far:
        unit(zs - 1, 0, last_g - 1, but=done)
        early = (z == 0) & (me < sp // 2)

        def first_parts():
            started.clear()
            weights_here()
            add_parts(range(last_g - 1))

        if square:
            each_z(plane_end)
        pl.when(early)(first_parts)
        each_z(far_below, lambda zz: zz in lower)
        unit(zs - 1, last_g - 1, last_g, but=done)
        unit(zs - 1, last_g, groups, but=lower + (zs - 1,))
        pl.when(jnp.logical_not(early))(first_parts)
        final = jnp.where(me == sp - 1, last_g - 1, last_g)
        add_parts([2 * last_g - 1 - final])
    elif groups > 1:
        if square:
            each_z(plane_end)
        weights_here()
        unit(zs - 1, 0, last_g, but=done)
        add_parts(range(last_g))
        unit(zs - 1, last_g, groups, but=(zs - 1,))
        final = last_g
    else:
        if square:
            each_z(plane_end)
        weights_here()
        unit(zs - 1, but=done)
        final = 0
    gather_part(final, not started)
    scale = lax.rsqrt(jnp.sum(sums_v[...], axis=-1, keepdims=True) / (sp * chans) + norm_eps)

    @pl.loop(0, width // step)
    def _(t):
        cols = pl.ds(pl.multiple_of(t * step, LANES), step)
        last = part_dot(final, cols)
        if started:
            last += part_v[:, cols]
        out_ref[:, cols] = (last * scale).astype(jnp.bfloat16)

    sent(tok_v.at[pl.ds(0, sp - 1)], tok_s.at[0])
    sent(outw_v.at[:, :, :, own_cols], ow_own.at[0])
    for r in range(1, sp):
        if not (square and r == 3):
            sent(ow_bytes(zs - 1), pl_s.at[r])
        sent(ow_bytes(zs - 1), pp_s.at[r])
    if square:
        sent(ow_bytes(zs - 1), p2_s.at[0])
    sent(ow_bytes(zs - 1), ow_send.at[2])
    sent(ug_v.at[pl.ds(0, zs * depth), :], ug_send.at[2])
    sent(held_v.at[pl.ds(0, sp - 1)], ga_s.at[0])

    def line_sent(zz):
        for n, way in ((zz + 1 if zz < zs - 1 else 0, 0), (zs - zz if zz > 0 else 0, 1)):
            if n:
                sent(ug_v.at[pl.ds(0, n * depth), :], ug_send.at[way])
                sent(ow_bytes(n), ow_send.at[way])
        if not inner(zz):
            n = sum(v_useful(zz, q) for q in range(sp))
            main = pl.ds(0, last_g if split(zz) else groups)
            sent(norm_v.at[main, pl.ds(0, n * per), :], v_s.at[0])
            if split(zz):
                sent(norm_v.at[pl.ds(0, 1), pl.ds(0, n * per), :], v_s.at[1])
        elif mate(zz) is not None:
            n = sum(with_mate(zz, o) for o in range(zs))
            sent(mixed_v.at[:, :, pl.ds(0, n)], ret_s.at[0])
        for i in range(2):
            if far and zz == below:
                sent(far_v.at[i], fv_s.at[i])
            if far and zz == above:
                sent(far_m.at[:, i], fm_s.at[i])

    each_z(line_sent)

    def mix_sent(zz, cc):
        for o in range(zs):
            d = o * CORES + cc
            for i, (r0, rn, cols) in enumerate(cuts(d)):
                spot = mix_v.at[:, d, pl.ds(r0, rn), pl.ds(0, cols)]
                if not (inner(zz) or o == zz):
                    continue
                if o >= zz and inner(zz - 1):
                    crossing = last_g if far and zz == above else groups
                    sent(mix_v.at[pl.ds(0, crossing), d, pl.ds(r0, rn), pl.ds(0, cols)],
                         mx_dn.at[o, i])
                if o <= zz and inner(zz + 1):
                    sent(spot, mx_up.at[o, i])
                paired = last_g if far and zz == below and o >= above else groups
                sent(mix_v.at[pl.ds(0, paired), d, pl.ds(r0, rn), pl.ds(0, cols)], mx_ps.at[o, i])

    each_d(mix_sent)


def body(tokens, up_weight, gate_weight, group_gain, mix_weight, mix_bias, out_gain, out_weight):
    per, width = tokens.shape[1:]
    groups, gd = group_gain.shape
    rows, block = mix_weight.shape[1:]
    sp, dps = lax.axis_size("sp"), lax.axis_size("dp")
    zs = dps // CORES
    total = sp * per
    parts = groups
    halves = 1 if parts % 2 else 2
    bf, f32 = jnp.bfloat16, jnp.float32
    dma = pltpu.SemaphoreType.DMA
    hbm = pl.BlockSpec(memory_space=pltpu.HBM)
    vmem = pl.BlockSpec(memory_space=pltpu.VMEM)
    output = pl.pallas_call(
        functools.partial(fused_kernel, sp, zs),
        out_shape=pltpu.VMEM((per, width), bf),
        in_specs=[hbm, hbm, hbm, vmem, hbm, vmem, vmem, hbm],
        out_specs=vmem,
        scratch_shapes=[
            pltpu.VMEM((sp, per, width), bf),
            pltpu.VMEM((width, 2 * groups * gd), bf),
            pltpu.VMEM((groups, dps, rows, block), bf),
            pltpu.VMEM((parts, sp, groups * gd // parts, width), bf),
            pltpu.VMEM((groups, total, gd), f32),
            pltpu.VMEM((groups, total, gd), bf),
            pltpu.VMEM((groups, total, gd), bf),
            pltpu.VMEM((groups, block, gd), f32),
            pltpu.VMEM((groups, total // block, zs, CORES * rows, gd), bf),
            pltpu.VMEM((groups, total, gd), bf),
            pltpu.VMEM((sp, groups, per, gd), bf),
            pltpu.VMEM((parts, per, sp * groups * gd // parts), bf),
            pltpu.VMEM((per, gd), f32),
            pltpu.VMEM((per, width if parts > 1 else gd), f32),
            pltpu.VMEM((2, total if parts > 2 else 16, gd), bf),
            pltpu.VMEM((2, 2, total // block, CORES * rows if parts > 2 else 16, gd), bf),
            dma((4,)),
            dma((zs, 2)), dma((3,)), dma((1,)),
            dma((zs,)), dma((3,)), dma((1,)), dma((2,)),
            dma((sp,)), dma((sp, zs)), dma((1,)), dma((zs, halves)), dma((sp,)), dma((sp,)),
            dma((groups, zs)), dma((groups, zs)), dma((zs, 2)), dma((zs, 2)), dma((zs, 2)),
            dma((1,)), dma((sp, 2)), dma((2,)), dma((2, sp)),
            dma((1,)), dma((groups, zs)), dma((1,)), dma((parts, sp)),
            dma((2,)), dma((2,)), dma((2,)), dma((2,)),
        ],
        compiler_params=pltpu.CompilerParams(collective_id=0, has_side_effects=True, vmem_limit_bytes=65_000_000),
    )(tokens.reshape(per, width), up_weight, gate_weight, group_gain[:, None, :], mix_weight, mix_bias,
      out_gain[None, :], out_weight.reshape(sp, parts, groups * gd // parts, -1))
    return output.reshape(tokens.shape)


def solution(mesh):
    return jax.shard_map(
        body,
        mesh=mesh,
        in_specs=(
            P("dp", "sp", None),
            P("dp", None),
            P("dp", None),
            P("sp", None),
            P("sp", "dp", None),
            P("sp", None),
            P(),
            P(None, "dp"),
        ),
        out_specs=P("dp", "sp", None),
        check_vma=False,
    )
```
